128 devices in a mesh: ep: 64 (over z, y, x), tp: 2 (over core).
Axes of the slice: x: 4, y: 4, z: 4, core: 2. Of those that a mesh axis runs over, the one named last changes fastest.
Arguments:
- tokens: bfloat16 [512, 2048], P('ep'), may hold values from -6 to 6
- mixer_norm_gain: float32 [2048], replicated, may hold values from 0.1 to 1.9
- gate_projection_weight: bfloat16 [2048, 2, 2048], P(None, 'tp', 'ep'), may hold values from -0.125 to 0.125
- value_projection_weight: bfloat16 [2048, 2, 2048], P(None, 'tp', 'ep'), may hold values from -0.125 to 0.125
- input_projection_weight: bfloat16 [2048, 1024], P(None, 'tp'), may hold values from -0.125 to 0.125
- output_projection_weight: bfloat16 [2048, 1024], P(None, 'tp'), may hold values from -0.125 to 0.125
- step_projection_weight: bfloat16 [2048, 64], P(None, 'tp'), may hold values from -0.125 to 0.125
- head_step_bias: float32 [64], P('tp'), may hold values from -1 to 1
- head_decay_rate: float32 [64], P('tp'), may hold values from 0.02 to 3
- extra_log_decay: float32 [512, 64], P('ep', 'tp'), may hold values from -0.7 to 0
- value_taps: float32 [4, 4096], P(None, 'tp'), may hold values from -3 to 3
- input_taps: float32 [4, 1024], P(None, 'tp'), may hold values from -3 to 3
- output_taps: float32 [4, 1024], P(None, 'tp'), may hold values from -3 to 3
- prior_values: bfloat16 [512, 3, 4096], P('ep', None, 'tp'), may hold values from -6 to 6
- prior_input_maps: bfloat16 [512, 3, 1024], P('ep', None, 'tp'), may hold values from -6 to 6
- prior_output_maps: bfloat16 [512, 3, 1024], P('ep', None, 'tp'), may hold values from -6 to 6
- head_skip_gain: float32 [64], P('tp'), may hold values from 0.5 to 1.5
- group_norm_gain: float32 [4096], P('tp'), may hold values from 0.1 to 1.9
- mixer_output_weight: bfloat16 [4096, 2048], P('tp', 'ep'), may hold values from -0.09375 to 0.09375
- recurrent_state: float32 [512, 64, 64, 128], P('ep', 'tp'), may hold values from -6 to 6
- expert_norm_gain: float32 [2048], replicated, may hold values from 0.1 to 1.9
- routes: int32 [512, 6], P('ep'), may hold values from 0 to 63, all different within a row; in each aligned block of 8 rows (0 to 7, 8 to 15, ...) at most 2 rows name the same one
- chosen_expert_weight: float32 [512, 6], P('ep'), may hold values from 0.2 to 1
- routed_gate_weight: bfloat16 [64, 2048, 512], P('ep', None, 'tp'), may hold values from -0.125 to 0.125
- routed_up_weight: bfloat16 [64, 2048, 512], P('ep', None, 'tp'), may hold values from -0.125 to 0.125
- routed_down_weight: bfloat16 [64, 512, 2048], P('ep', 'tp'), may hold values from -0.25 to 0.25
- common_gate_weight: bfloat16 [2048, 512], P(None, 'tp'), may hold values from -0.125 to 0.125
- common_up_weight: bfloat16 [2048, 512], P(None, 'tp'), may hold values from -0.125 to 0.125
- common_down_weight: bfloat16 [512, 2048], P('tp'), may hold values from -0.25 to 0.25
Outputs:
- result: bfloat16 [512, 2048], P('ep')
- state_next: float32 [512, 64, 64, 128], P('ep', 'tp')
- next_value: bfloat16 [512, 3, 4096], P('ep', None, 'tp')
- next_input: bfloat16 [512, 3, 1024], P('ep', None, 'tp')
- next_output: bfloat16 [512, 3, 1024], P('ep', None, 'tp')
The draws below stay inside these ranges and needn't reach their ends.
Inputs may be any that keep to these rules, and one draw needn't show every extreme that they name: `routes`: the 6 experts of a row differ; among the rows of one device (aligned blocks of 8 rows) no expert is named more than 2 times.
All inputs are finite; a program needn't handle non-finite values.
Results may differ from the reference program's by a relative error of at most 0.015.
Values may be sent and summed in bfloat16 or wider, within the bound.
A program may use at most 128 MiB of HBM per device.

```python
import math
import jax
import jax.numpy as jnp
import numpy as np
from jax import lax

D = 2048
D_INNER = 4096
HEAD = 64
MIXER_HEADS = 64
STATE = 128
GROUPS = 8
CONV = 4
FE = 512
FS = 512
TOPK = 6
EXPERTS = 64
SEQ_DEV = 8
SEQUENCE_COUNT = 512
CAP = 2
HALF = 2048
N_EP = 64
N_TP = 2


def shard_levels(stream_key, dims, pieces, least, top_value):
    def one(dim, blocks):
        heights = jax.random.uniform(jax.random.fold_in(jax.random.fold_in(stream_key, 6), dim), (blocks,), jnp.float32, least / len(pieces), top_value / len(pieces))
        return jnp.repeat(jnp.exp(heights), dims[dim] // blocks).reshape((-1,) + (1,) * (len(dims) - dim - 1))

    level = one(*pieces[0])
    for cut in pieces[1:]:
        level = level * one(*cut)
    return level


def deal_out(rng, own, number, rows, amount, top, reach, slope):
    order = jax.random.permutation(rng, amount)
    crowded, ordinary = load_shares(amount, rows * top, reach, slope, True), load_shares(amount, rows * top, reach, slope, False)
    places = jnp.arange(amount)

    def named(sizes, offset_by):
        used = int((sizes > 0).sum())
        fixed = max(1, used // 4)
        passed = fixed + (places - fixed + offset_by * (used - fixed)) % max(1, amount - fixed)
        return jnp.zeros((amount,), jnp.int32).at[order[jnp.where(places < fixed, places, passed)]].set(jnp.asarray(sizes, jnp.int32))

    sizes = jnp.where(number % 4 == 0, named(crowded, number // 4), named(ordinary, number - number // 4 - 1))
    mixed = jax.random.permutation(jax.random.fold_in(own, 3), amount)
    donor, taker = mixed[0:amount // 2 * 2:2], mixed[1:amount // 2 * 2:2]
    margin = jnp.minimum(sizes[donor] - 1, reach - sizes[taker]) // 2
    margin = jnp.where((donor == order[0]) | (taker == order[0]) | (sizes[taker] == 0), 0, jnp.maximum(margin, 0))
    passed = jax.random.randint(jax.random.fold_in(own, 4), (amount // 2,), 0, 1 << 20) % (margin + 1)
    sizes = sizes.at[donor].add(-passed).at[taker].add(passed)
    items = jnp.searchsorted(jnp.cumsum(sizes), jnp.arange(rows * top), side="right").astype(jnp.int32)
    grid = items.reshape(top, rows).T
    grid = grid[jax.random.permutation(jax.random.fold_in(own, 1), rows)]
    offset_by = jax.random.randint(jax.random.fold_in(own, 2), (rows, 1), 0, top)
    return jnp.take_along_axis(grid, (jnp.arange(top)[None, :] + offset_by) % top, axis=1)


def load_shares(count, total, reach, slope, full):
    portions = [(1 << 20) // math.isqrt(standing ** slope) + 1 for standing in range(1, count + 1)]
    largest = reach if full else min(reach, max(-(-total // count), total * portions[0] // sum(portions)))
    least = 1 if total - largest >= count - 1 else 0
    given, surplus = [largest] + [least] * (count - 1), total - largest - least * (count - 1)
    while surplus > 0:
        free = [i for i in range(1, count) if given[i] < largest] or [i for i in range(1, count) if given[i] < reach]
        pool, left = sum([portions[i] for i in free]), surplus
        for i in free:
            addition = min(reach - given[i], max(1, left * portions[i] // pool), surplus)
            given[i] = given[i] + addition
            surplus = surplus - addition
    return np.array(given)


def gaussian(key, shape, spread, limit, cuts=(), kind=jnp.bfloat16):
    drawn = spread * jax.random.normal(key, shape, jnp.float32)
    if cuts:
        drawn = drawn * shard_levels(key, shape, cuts, -0.22, 0.18)
    return jnp.clip(drawn, -limit, limit).astype(kind)


def setup_inputs(seed: int = 0) -> dict:
    key_list = jax.random.split(jax.random.key(seed), 30)
    tokens = gaussian(key_list[0], (SEQUENCE_COUNT, D), 1.0, 6.0, ((0, 64),))
    mixer_norm_gain = jnp.clip(1.0 + 0.18 * jax.random.normal(key_list[1], (D,), jnp.float32), 0.1, 1.9)
    gate_projection_weight = gaussian(key_list[2], (D, N_TP, HALF), D ** -0.5, 0.125, ((1, 2), (2, 64)))
    value_projection_weight = gaussian(key_list[3], (D, N_TP, HALF), D ** -0.5, 0.125, ((1, 2), (2, 64)))
    input_projection_weight = gaussian(key_list[4], (D, GROUPS * STATE), D ** -0.5, 0.125, ((1, 2),))
    output_projection_weight = gaussian(key_list[5], (D, GROUPS * STATE), D ** -0.5, 0.125, ((1, 2),))
    step_projection_weight = gaussian(key_list[6], (D, MIXER_HEADS), D ** -0.5, 0.125, ((1, 2),))
    head_step_bias = jnp.clip(jax.random.uniform(key_list[7], (MIXER_HEADS,), jnp.float32, -1.0, 1.0) * shard_levels(key_list[7], (MIXER_HEADS,), ((0, 2),), -0.4, 0.0), -1.0, 1.0)
    head_decay_rate = jnp.clip(jnp.exp(math.log(3.0) - 5.0106353 * jax.random.uniform(key_list[8], (MIXER_HEADS,), jnp.float32) ** shard_levels(key_list[8], (MIXER_HEADS,), ((0, 2),), -0.2, 0.2)), 0.02, 3.0)
    extra_log_decay = jnp.clip(-0.7 + 0.7 * jax.random.uniform(key_list[9], (SEQUENCE_COUNT, MIXER_HEADS), jnp.float32) ** shard_levels(key_list[9], (SEQUENCE_COUNT, MIXER_HEADS), ((0, 64), (1, 2)), -0.2, 0.2), -0.7, 0.0)
    value_taps = gaussian(key_list[10], (CONV, D_INNER), 0.5, 3.0, ((1, 2),), jnp.float32)
    input_taps = gaussian(key_list[11], (CONV, GROUPS * STATE), 0.5, 3.0, ((1, 2),), jnp.float32)
    output_taps = gaussian(key_list[12], (CONV, GROUPS * STATE), 0.5, 3.0, ((1, 2),), jnp.float32)
    prior_values = gaussian(key_list[13], (SEQUENCE_COUNT, CONV - 1, D_INNER), 1.0, 6.0, ((0, 64), (2, 2)))
    prior_input_maps = gaussian(key_list[14], (SEQUENCE_COUNT, CONV - 1, GROUPS * STATE), 1.0, 6.0, ((0, 64), (2, 2)))
    prior_output_maps = gaussian(key_list[15], (SEQUENCE_COUNT, CONV - 1, GROUPS * STATE), 1.0, 6.0, ((0, 64), (2, 2)))
    head_skip_gain = jnp.clip(0.5 + 1.0 * jax.random.uniform(key_list[16], (MIXER_HEADS,), jnp.float32) ** shard_levels(key_list[16], (MIXER_HEADS,), ((0, 2),), -0.2, 0.2), 0.5, 1.5)
    group_norm_gain = jnp.clip(1.0 + 0.18 * jax.random.normal(key_list[17], (D_INNER,), jnp.float32), 0.1, 1.9)
    mixer_output_weight = gaussian(key_list[18], (D_INNER, D), D_INNER ** -0.5, 0.09375, ((0, 2), (1, 64)))
    recurrent_state = gaussian(key_list[19], (SEQUENCE_COUNT, MIXER_HEADS, HEAD, STATE), 1.0, 6.0, ((0, 64), (1, 2)), jnp.float32)
    expert_norm_gain = jnp.clip(1.0 + 0.18 * jax.random.normal(key_list[20], (D,), jnp.float32), 0.1, 1.9)
    routes_keys = jax.random.split(jax.random.fold_in(key_list[21], 1), SEQUENCE_COUNT // SEQ_DEV)
    routes_turns = jax.random.permutation(jax.random.fold_in(key_list[21], 3), SEQUENCE_COUNT // SEQ_DEV)
    routes = jax.vmap(lambda own, number: deal_out(jax.random.fold_in(key_list[21], 2), own, number, SEQ_DEV, EXPERTS, TOPK, CAP, 1))(routes_keys, routes_turns).reshape((SEQUENCE_COUNT, TOPK))
    chosen_expert_weight = jnp.clip(0.2 + 0.8 * jax.random.uniform(key_list[22], (SEQUENCE_COUNT, TOPK), jnp.float32) ** shard_levels(key_list[22], (SEQUENCE_COUNT, TOPK), ((0, 64),), -0.2, 0.2), 0.2, 1.0)
    routed_gate_weight = gaussian(key_list[23], (EXPERTS, D, FE), D ** -0.5, 0.125, ((0, 64), (2, 2)))
    routed_up_weight = gaussian(key_list[24], (EXPERTS, D, FE), D ** -0.5, 0.125, ((0, 64), (2, 2)))
    routed_down_weight = gaussian(key_list[25], (EXPERTS, FE, D), FE ** -0.5, 0.25, ((0, 64), (1, 2)))
    common_gate_weight = gaussian(key_list[26], (D, FS), D ** -0.5, 0.125, ((1, 2),))
    common_up_weight = gaussian(key_list[27], (D, FS), D ** -0.5, 0.125, ((1, 2),))
    common_down_weight = gaussian(key_list[28], (FS, D), FS ** -0.5, 0.25, ((0, 2),))
    return dict(tokens=tokens, mixer_norm_gain=mixer_norm_gain, gate_projection_weight=gate_projection_weight, value_projection_weight=value_projection_weight, input_projection_weight=input_projection_weight, output_projection_weight=output_projection_weight, step_projection_weight=step_projection_weight, head_step_bias=head_step_bias, head_decay_rate=head_decay_rate, extra_log_decay=extra_log_decay, value_taps=value_taps, input_taps=input_taps, output_taps=output_taps, prior_values=prior_values, prior_input_maps=prior_input_maps, prior_output_maps=prior_output_maps, head_skip_gain=head_skip_gain, group_norm_gain=group_norm_gain, mixer_output_weight=mixer_output_weight, recurrent_state=recurrent_state, expert_norm_gain=expert_norm_gain, routes=routes, chosen_expert_weight=chosen_expert_weight, routed_gate_weight=routed_gate_weight, routed_up_weight=routed_up_weight, routed_down_weight=routed_down_weight, common_gate_weight=common_gate_weight, common_up_weight=common_up_weight, common_down_weight=common_down_weight)


EPSILON = 1e-06

def rms_scale(values, gain_vec):
    values = values.astype(jnp.float32)
    return values * lax.rsqrt(lax.optimization_barrier(jnp.mean(values * values, axis=-1, keepdims=True)) + EPSILON) * gain_vec

def short_conv(past_rows, fresh_row, weight):
    window = jnp.concatenate([past_rows, fresh_row[:, None, :]], axis=1)
    summed = window[:, 0].astype(jnp.float32) * weight[0]
    for offset in range(1, window.shape[1]):
        summed = summed + window[:, offset].astype(jnp.float32) * weight[offset]
    return (jax.nn.silu(summed), window[:, 1:])

def state_step(state_prev, value_conv, input_conv, output_conv, timestep_size, step_decay, head_skip_gain):
    batch_rows, head_count, head_size, state_size = state_prev.shape
    per_group = head_count // (input_conv.shape[1] // state_size)
    value_heads = value_conv.reshape(batch_rows, head_count, head_size)
    input_heads = jnp.repeat(input_conv.reshape(batch_rows, -1, state_size), per_group, axis=1)
    output_heads = jnp.repeat(output_conv.reshape(batch_rows, -1, state_size), per_group, axis=1)
    state_next = step_decay[:, :, None, None] * state_prev + (timestep_size[:, :, None] * value_heads)[:, :, :, None] * input_heads[:, :, None, :]
    mixed_heads = lax.optimization_barrier(jnp.sum(state_next * output_heads[:, :, None, :], axis=-1)) + head_skip_gain[None, :, None] * value_heads
    return (state_next, mixed_heads.reshape(batch_rows, -1))

def gated_norm(mixed_flat, gate_rows, group_norm_gain, group_width):
    gated_rows = mixed_flat * jax.nn.silu(gate_rows.astype(jnp.float32))
    grouped = gated_rows.reshape(gated_rows.shape[0], -1, group_width)
    grouped = grouped * lax.rsqrt(lax.optimization_barrier(jnp.mean(grouped * grouped, axis=-1, keepdims=True)) + EPSILON)
    return (grouped.reshape(gated_rows.shape[0], -1) * group_norm_gain).astype(jnp.bfloat16)

def half_sum(left_rows, right_matrix, halves):
    span_width = left_rows.shape[1] // halves
    summed = jnp.zeros((left_rows.shape[0], right_matrix.shape[1]), jnp.float32)
    for half_index in range(halves):
        partial_value = jnp.dot(left_rows[:, half_index * span_width:(half_index + 1) * span_width], right_matrix[half_index * span_width:(half_index + 1) * span_width], preferred_element_type=jnp.float32)
        rounded = lax.optimization_barrier(partial_value.astype(jnp.bfloat16))
        summed = summed + rounded.astype(jnp.float32)
    return summed

def reference(tokens, mixer_norm_gain, gate_projection_weight, value_projection_weight, input_projection_weight, output_projection_weight, step_projection_weight, head_step_bias, head_decay_rate, extra_log_decay, value_taps, input_taps, output_taps, prior_values, prior_input_maps, prior_output_maps, head_skip_gain, group_norm_gain, mixer_output_weight, recurrent_state, expert_norm_gain, routes, chosen_expert_weight, routed_gate_weight, routed_up_weight, routed_down_weight, common_gate_weight, common_up_weight, common_down_weight):
    normed = rms_scale(tokens, mixer_norm_gain).astype(jnp.bfloat16)
    gate_rows = jnp.dot(normed, gate_projection_weight.reshape(D, D_INNER), preferred_element_type=jnp.float32).astype(jnp.bfloat16)
    value_rows = jnp.dot(normed, value_projection_weight.reshape(D, D_INNER), preferred_element_type=jnp.float32).astype(jnp.bfloat16)
    input_rows = jnp.dot(normed, input_projection_weight, preferred_element_type=jnp.float32).astype(jnp.bfloat16)
    output_rows = jnp.dot(normed, output_projection_weight, preferred_element_type=jnp.float32).astype(jnp.bfloat16)
    step_raw = jnp.dot(normed, step_projection_weight, preferred_element_type=jnp.float32)
    value_conv, next_value = short_conv(prior_values, value_rows, value_taps)
    input_conv, next_input = short_conv(prior_input_maps, input_rows, input_taps)
    output_conv, next_output = short_conv(prior_output_maps, output_rows, output_taps)
    timestep_size = jax.nn.softplus(step_raw + head_step_bias)
    step_decay = jnp.exp(-timestep_size * head_decay_rate + extra_log_decay)
    state_next, mixed_flat = state_step(recurrent_state, value_conv, input_conv, output_conv, timestep_size, step_decay, head_skip_gain)
    mixer_rows = gated_norm(mixed_flat, gate_rows, group_norm_gain, D_INNER // GROUPS)
    mixed_out = half_sum(mixer_rows, mixer_output_weight, N_TP).astype(jnp.bfloat16)
    stream = (tokens.astype(jnp.float32) + mixed_out.astype(jnp.float32)).astype(jnp.bfloat16)
    ffn_rows = rms_scale(stream, expert_norm_gain).astype(jnp.bfloat16)
    shared_hidden = (jax.nn.silu(jnp.dot(ffn_rows, common_gate_weight, preferred_element_type=jnp.float32)) * jnp.dot(ffn_rows, common_up_weight, preferred_element_type=jnp.float32)).astype(jnp.bfloat16)
    shared_out = half_sum(shared_hidden, common_down_weight, N_TP)
    flat_routes = routes.reshape(N_EP, SEQ_DEV * TOPK)
    expert_ids = jnp.arange(EXPERTS, dtype=jnp.int32)
    onehot = (flat_routes[:, :, None] == expert_ids[None, None, :]).astype(jnp.int32)
    slot_ids = lax.optimization_barrier(jnp.sum((jnp.cumsum(onehot, axis=1) - onehot) * onehot, axis=2)).astype(jnp.int32)
    device_ids = jnp.broadcast_to(jnp.arange(N_EP, dtype=jnp.int32)[:, None], flat_routes.shape)
    token_ids = device_ids * SEQ_DEV + jnp.broadcast_to(jnp.arange(SEQ_DEV * TOPK, dtype=jnp.int32)[None, :] // TOPK, flat_routes.shape)
    slot_table = jnp.full((EXPERTS, N_EP, CAP), SEQUENCE_COUNT, jnp.int32).at[flat_routes, device_ids, slot_ids].set(token_ids)
    padded = jnp.concatenate([ffn_rows, jnp.zeros((1, D), jnp.bfloat16)], axis=0)

    def per_expert(operands):
        index_table, gate_mat, up_mat, down_mat = operands
        picked_rows = padded[index_table.reshape(-1)]
        hidden = (jax.nn.silu(jnp.dot(picked_rows, gate_mat, preferred_element_type=jnp.float32)) * jnp.dot(picked_rows, up_mat, preferred_element_type=jnp.float32)).astype(jnp.bfloat16)
        return half_sum(hidden, down_mat, N_TP).astype(jnp.bfloat16).reshape(N_EP, CAP, D)
    expert_out = lax.map(per_expert, (slot_table, routed_gate_weight, routed_up_weight, routed_down_weight))
    picked = expert_out[flat_routes, device_ids, slot_ids].astype(jnp.float32)
    weighted = picked * chosen_expert_weight.reshape(N_EP, SEQ_DEV * TOPK)[:, :, None]
    routed = lax.optimization_barrier(jnp.sum(weighted.reshape(SEQUENCE_COUNT, TOPK, D), axis=1))
    result = (stream.astype(jnp.float32) + shared_out + routed).astype(jnp.bfloat16)
    return (result, state_next, next_value, next_input, next_output)
```

```python
import functools

import jax
import jax.numpy as jnp
from jax import lax
from jax.experimental import pallas as pl
from jax.experimental.pallas import tpu as pltpu
from jax.sharding import PartitionSpec as P

MESH = pl.DeviceIdType.MESH
EPSILON = 1e-06
BF, F32 = jnp.bfloat16, jnp.float32
NT = (((1,), (1,)), ((), ()))
TN = (((0,), (0,)), ((), ()))
HALF = 1024
PIECES = ((0, 256), (256, 384), (640, 384))

SEM_A = 0
SEM_B = SEM_A + 48
SEM_F = SEM_B + 9
SEM_P = SEM_F + 3
SEM_W = SEM_P + 64
SEM_M = SEM_W + 3
SEM_Q = SEM_M + 16
SEM_X = SEM_Q + 32
SEM_Y = SEM_X + 64
SEM_FX = SEM_Y + 64
SEM_SH = SEM_FX + 1
SEM_YE = SEM_SH + 1
SEM_RF = SEM_YE + 1
SEM_COUNT = SEM_RF + 1

LOADED = (
    "tok", "g1", "wi", "wo", "wst", "sb", "dr", "eld", "vt", "it", "ot", "pv", "pi", "po", "hs",
    "gg", "g2", "routes", "cw", "rg", "ru", "rd", "cg", "cu", "cd", "st",
)


def silu(x):
    return x * (1.0 / (1.0 + jnp.exp(-x)))


def rms(x, gain):
    return x * lax.rsqrt(jnp.mean(x * x, axis=-1, keepdims=True) + EPSILON) * gain


def split_bf(x):
    hi = x.astype(BF)
    return hi, (x - hi.astype(F32)).astype(BF)


def dot(a, b, dims=(((1,), (0,)), ((), ()))):
    return lax.dot_general(a, b, dims, preferred_element_type=F32)


def lane_groups(pieces, lane):
    return jnp.where(
        lane < 32,
        pieces[0],
        jnp.where(lane < 64, pieces[1], jnp.where(lane < 96, pieces[2], pieces[3])),
    )


def layer_kernel(*refs):
    hbm = dict(zip(LOADED + ("gt", "vtp", "wmt"), refs[:29]))
    res_o, st_o, nv_o, ni_o, no_o = refs[29:34]
    v = dict(zip(LOADED, refs[34:60]))
    (
        X, WGV, WM, SP, R1, M, SQ, R2, SD, RX, XF, YS, YR, SY, RY, SHS, SHR, RES, RESR, DM, CM, QR,
        CC, FF, BV, DV, UT, ld, ss, rs,
    ) = refs[60:]

    e = lax.axis_index("ep")
    c = lax.axis_index("tp")
    oc = 1 - c
    z, y, x = e // 16, (e // 4) % 4, e % 4
    own = (z, y, x)

    def ep_of(zz, yy, xx):
        return zz * 16 + yy * 4 + xx

    def send(src, dst, so, ro, dev):
        return pltpu.make_async_remote_copy(
            src_ref=src, dst_ref=dst, send_sem=ss.at[so], recv_sem=rs.at[ro],
            device_id=dev, device_id_type=MESH,
        )

    def got(dst, ro):
        send(dst, dst, ro, ro, (e, oc)).wait_recv()

    def sent(src, so):
        send(src, src, so, so, (e, oc)).wait_send()

    pending = []

    def finish():
        for f in pending:
            f()

    loads = {}
    for k, n in enumerate(LOADED):
        loads[n] = pltpu.make_async_copy(hbm[n], v[n], ld.at[k])
    base = len(LOADED)
    gcopy = pltpu.make_async_copy(hbm["gt"], WGV.at[x], ld.at[base])
    vcopies = [
        pltpu.make_async_copy(hbm["vtp"], WGV.at[(x + 1 + j) % 4], ld.at[base + 1 + j])
        for j in range(3)
    ]
    wcopy = pltpu.make_async_copy(hbm["wmt"], WM.at[z], ld.at[base + 4])
    loads["tok"].start()
    loads["g1"].start()
    wcopy.start()
    loads["wst"].start()
    for n in ("wi", "wo", "sb", "dr", "eld", "vt", "it", "ot", "pv", "pi", "po", "hs", "gg", "g2", "routes", "cw"):
        loads[n].start()
    gcopy.start()
    for w in vcopies:
        w.start()
    for n in ("st", "cg", "cu", "cd", "rg", "ru", "rd"):
        loads[n].start()

    bar = pltpu.get_barrier_semaphore()
    pl.semaphore_signal(bar, inc=1, device_id=(e, oc), device_id_type=MESH)

    def sig_all(k, _):
        pl.semaphore_signal(
            bar, inc=1, device_id=(lax.rem(e + 1 + k, 64), c), device_id_type=MESH
        )
        return 0

    lax.fori_loop(0, 63, sig_all, 0)
    p_own = y * 4 + x

    def sig_plane(k, _):
        pl.semaphore_signal(
            bar, inc=1, device_id=(z * 16 + lax.rem(p_own + 1 + k, 16), oc), device_id_type=MESH
        )
        return 0

    lax.fori_loop(0, 15, sig_plane, 0)

    loads["tok"].wait()
    loads["g1"].wait()
    tok = v["tok"][...].astype(F32)
    normed = rms(tok, v["g1"][...]).astype(BF)
    nf = normed.astype(F32)
    X[c, z, y, x] = jnp.where(c == 0, nf[:, :HALF], nf[:, HALF:]).astype(BF)

    pl.semaphore_wait(bar, 79)

    def coords(i, line, p):
        a, b = p // 4, p % 4
        return ((line, a, b), (a, line, b), (a, b, line))[i]

    def plane_index(i):
        return (y * 4 + x, z * 4 + x, z * 4 + y)[i]

    def cols(i):
        return pl.ds(PIECES[i][0], PIECES[i][1])

    def own_piece(i):
        return X.at[c, z, y, x, :, cols(i)]

    def a_send(k, _):
        for i in range(3):
            p = plane_index(i)
            q = lax.rem(p + 1 + k, 16)
            dev = (ep_of(*coords(i, own[i], q)), c)
            send(own_piece(i), own_piece(i), SEM_A + i * 16 + q, SEM_A + i * 16 + p, dev).start()
        return 0

    lax.fori_loop(0, 15, a_send, 0)

    def a_sent(k, _):
        for i in range(3):
            q = lax.rem(plane_index(i) + 1 + k, 16)
            sent(own_piece(i), SEM_A + i * 16 + q)
        return 0

    pending.append(lambda: lax.fori_loop(0, 15, a_sent, 0))

    wcopy.wait()
    for d in range(1, 4):
        dev = (ep_of((z + d) % 4, y, x), c)
        send(WM.at[z], WM.at[z], SEM_W + d - 1, SEM_W + d - 1, dev).start()
        pending.append(lambda d=d: sent(WM.at[z], SEM_W + d - 1))

    for n in ("wi", "wo", "wst", "sb", "dr", "eld", "it", "ot", "pi", "po"):
        loads[n].wait()
    in_rows = dot(normed, v["wi"][...]).astype(BF)
    out_rows = dot(normed, v["wo"][...]).astype(BF)
    step_raw = dot(normed, v["wst"][...], NT)

    def conv(prior, fresh, taps):
        t = taps[...]
        total = fresh * t[3:4]
        for j in range(3):
            total = total + prior[j].astype(F32) * t[j : j + 1]
        return silu(total)

    b_conv = conv(v["pi"], in_rows.astype(F32), v["it"])
    c_conv = conv(v["po"], out_rows.astype(F32), v["ot"])
    BV[...] = b_conv
    pre = step_raw + v["sb"][...]
    dt = jnp.maximum(pre, 0.0) + jnp.log(1.0 + jnp.exp(-jnp.abs(pre)))
    dec = jnp.exp(-dt * v["dr"][...] + v["eld"][...])
    c_hi, c_lo = split_bf(c_conv)
    CC[...] = jnp.concatenate([c_hi.astype(F32), c_lo.astype(F32)], axis=0).astype(BF)

    def plane_of(i):
        if i == 0:
            return X.at[c, z, :, :, :, cols(i)]
        if i == 1:
            return X.at[c, :, y, :, :, cols(i)]
        return X.at[c, :, :, x, :, cols(i)]

    def plane_from(i, line):
        if i == 0:
            return X.at[c, line, :, :, :, cols(i)]
        if i == 1:
            return X.at[c, :, line, :, :, cols(i)]
        return X.at[c, :, :, line, :, cols(i)]

    def a_got(k, _):
        for i in range(3):
            q = lax.rem(plane_index(i) + 1 + k, 16)
            zz, yy, xx = coords(i, own[i], q)
            got(X.at[c, zz, yy, xx, :, cols(i)], SEM_A + i * 16 + q)
        return 0

    lax.fori_loop(0, 15, a_got, 0)
    for d in range(1, 4):
        for i in range(3):
            there = list(own)
            there[i] = (own[i] + d) % 4
            send(
                plane_of(i), plane_of(i), SEM_B + i * 3 + d - 1, SEM_B + i * 3 + d - 1,
                (ep_of(*there), c),
            ).start()
            pending.append(lambda i=i, d=d: sent(plane_of(i), SEM_B + i * 3 + d - 1))

    loads["st"].wait()
    row = lax.broadcasted_iota(jnp.int32, (8, 512), 0)
    QR[...] = jnp.zeros((8, 2048), F32)

    def q_step(b, _):
        for g in range(4):
            s = v["st"][b, g * 512 : (g + 1) * 512, :].astype(BF)
            r = dot(CC[:, g * 128 : (g + 1) * 128], s, NT)
            sl = pl.ds(g * 512, 512)
            QR[:, sl] = jnp.where(row == b, r[0:8] + r[8:16], QR[:, sl])
        return 0

    lax.fori_loop(0, 8, q_step, 0)

    d1 = dec.astype(BF)
    d2 = (dec - d1.astype(F32)).astype(BF)
    seq = lax.broadcasted_iota(jnp.int32, (8, 1024), 1) // 128
    ones = (seq == lax.broadcasted_iota(jnp.int32, (8, 1024), 0)).astype(BF)
    spread_dec = dot(d1, ones, TN) + dot(d2, ones, TN)
    for b in range(8):
        DV[b] = spread_dec[:, b * 128 : (b + 1) * 128]

    loads["hs"].wait()
    spread = (
        lax.broadcasted_iota(jnp.int32, (32, 2048), 1) // 64
        == lax.broadcasted_iota(jnp.int32, (32, 2048), 0)
    ).astype(BF)
    heads = jnp.concatenate([dt, dec, jnp.broadcast_to(v["hs"][...], (8, 32))], axis=0)
    h1 = heads.astype(BF)
    r1 = heads - h1.astype(F32)
    h2 = r1.astype(BF)
    h3 = (r1 - h2.astype(F32)).astype(BF)
    wide = dot(h1, spread) + dot(h2, spread) + dot(h3, spread)
    dt_w, dec_w, skip_w = wide[0:8], wide[8:16], wide[16:24]
    bc = b_conv * c_conv
    bc_w = jnp.concatenate(
        [
            jnp.broadcast_to(
                jnp.sum(bc[:, g * 128 : (g + 1) * 128], axis=1, keepdims=True), (8, 512)
            )
            for g in range(4)
        ],
        axis=1,
    )
    kept = dec_w * QR[...]
    v_gain = dt_w * bc_w + skip_w

    for i in range(3):
        for d in range(1, 4):
            got(plane_from(i, (own[i] + 4 - d) % 4), SEM_B + i * 3 + d - 1)
        send(
            X.at[c, :, :, :, :, cols(i)], X.at[c, :, :, :, :, cols(i)], SEM_F + i, SEM_F + i,
            (e, oc),
        ).start()
        pending.append(lambda i=i: sent(X.at[c, :, :, :, :, cols(i)], SEM_F + i))
    gcopy.wait()
    for w in vcopies:
        w.wait()
    for i in range(3):
        got(X.at[oc, :, :, :, :, cols(i)], SEM_F + i)
    proj = dot(
        X[0].reshape(512, HALF), WGV[:, :, :HALF].reshape(128, HALF), NT
    ) + dot(X[1].reshape(512, HALF), WGV[:, :, HALF:].reshape(128, HALF), NT)
    SP[...] = proj.reshape(64, 8, 128).astype(BF)

    def p_send(k, _):
        q = lax.rem(e + 1 + k, 64)
        send(SP.at[q], R1.at[e], SEM_P + q, SEM_P + e, (q, c)).start()
        return 0

    lax.fori_loop(0, 63, p_send, 0)

    def p_sent(k, _):
        q = lax.rem(e + 1 + k, 64)
        sent(SP.at[q], SEM_P + q)
        return 0

    pending.append(lambda: lax.fori_loop(0, 63, p_sent, 0))
    R1[e] = SP[e]

    loads["routes"].wait()
    loads["cw"].wait()
    lane8 = lax.broadcasted_iota(jnp.int32, (8, 128), 1)
    hit = jnp.zeros((8, 128), F32)
    wgt = jnp.zeros((8, 128), F32)
    rt = v["routes"][...]
    cwv = v["cw"][...]
    for k in range(6):
        eq = lane8 == rt[:, k : k + 1]
        hit = hit + jnp.where(eq, 1.0, 0.0)
        wgt = wgt + jnp.where(eq, cwv[:, k : k + 1], 0.0)
    before = (
        lax.broadcasted_iota(jnp.int32, (8, 8), 0) > lax.broadcasted_iota(jnp.int32, (8, 8), 1)
    ).astype(BF)
    slot = dot(before, hit.astype(BF))
    s0 = jnp.where(slot < 0.5, 1.0, 0.0)
    w1 = wgt.astype(BF).astype(F32)
    w2 = wgt - w1
    rows6 = jnp.concatenate(
        [hit * s0, hit * (1 - s0), w1 * s0, w1 * (1 - s0), w2 * s0, w2 * (1 - s0)], axis=0
    ).astype(BF)
    place = (
        lax.broadcasted_iota(jnp.int32, (128, 1024), 1) // 16
        == lax.broadcasted_iota(jnp.int32, (128, 1024), 0)
    ).astype(BF)
    six = dot(rows6, place)
    lane_r = lax.broadcasted_iota(jnp.int32, (8, 1024), 1)
    first = (lane_r // 8) % 2 == 0
    hsel = jnp.where(first, six[0:8], six[8:16])
    w1s = jnp.where(first, six[16:24], six[24:32])
    w2s = jnp.where(first, six[32:40], six[40:48])
    tile = lane_r % 8
    zero = jnp.zeros((8, 1024), F32)

    def diag(a):
        return jnp.concatenate([jnp.where(tile == j, a, zero) for j in range(8)], axis=0)

    DM[...] = jnp.concatenate([diag(hsel), jnp.zeros((64, 1024), F32)], axis=0).T.astype(BF)
    CM[...] = jnp.concatenate([diag(w1s), diag(w2s)], axis=0).astype(BF)
    for n in ("vt", "pv", "gg"):
        loads[n].wait()

    def p_got(k, _):
        q = lax.rem(e + 1 + k, 64)
        got(R1.at[q], SEM_P + q)
        return 0

    lax.fori_loop(0, 63, p_got, 0)

    gates, values = [], []
    for t in range(16):
        r = [R1[4 * t + j].astype(F32) for j in range(4)]
        gates.append(lane_groups(r, lane8))
        values.append(pltpu.roll(lane_groups([r[3], r[0], r[1], r[2]], lane8), 96, 1))
    gate = jnp.concatenate(gates, axis=1)
    value = jnp.concatenate(values, axis=1)
    value_rows = value.astype(BF)
    v_conv = conv(v["pv"], value, v["vt"])
    mixed = (kept + v_conv * v_gain) * silu(gate)
    normed_groups = []
    for g in range(4):
        m = mixed[:, g * 512 : (g + 1) * 512]
        normed_groups.append(m * lax.rsqrt(jnp.mean(m * m, axis=1, keepdims=True) + EPSILON))
    mixer_rows = jnp.concatenate(normed_groups, axis=1) * v["gg"][...]
    M[y, x] = mixer_rows.astype(BF)

    def m_send(k, _):
        q = lax.rem(p_own + 1 + k, 16)
        send(M.at[y, x], M.at[y, x], SEM_M + q, SEM_M + p_own, (z * 16 + q, c)).start()
        return 0

    lax.fori_loop(0, 15, m_send, 0)

    def m_sent(k, _):
        sent(M.at[y, x], SEM_M + lax.rem(p_own + 1 + k, 16))
        return 0

    pending.append(lambda: lax.fori_loop(0, 15, m_sent, 0))
    for new, old, fresh in ((nv_o, "pv", value_rows), (ni_o, "pi", in_rows), (no_o, "po", out_rows)):
        new[0] = v[old][1]
        new[1] = v[old][2]
        new[2] = fresh

    u = v_conv * dt_w
    u1 = u.astype(BF).astype(F32)
    pad = jnp.zeros((104, 2048), F32)
    UT[...] = jnp.concatenate([u1, u1, u - u1, pad], axis=0).T.astype(BF)

    def st_step(b, _):
        bv = BV[...]
        b1 = bv.astype(BF).astype(F32)
        keep = lax.broadcasted_iota(jnp.int32, (8, 512), 0) == b
        zero = jnp.zeros((8, 512), F32)
        k1, k2 = jnp.where(keep, b1, zero), jnp.where(keep, bv - b1, zero)
        rhs = jnp.concatenate([k1, k2, k1, jnp.zeros((104, 512), F32)], axis=0).astype(BF)
        for g in range(4):
            outer = dot(UT[g * 512 : (g + 1) * 512, :], rhs[:, g * 128 : (g + 1) * 128])
            for h in range(8):
                sl = pl.ds(g * 512 + h * 64, 64)
                keep_h = DV[b, pl.ds(g * 8 + h, 1), :]
                st_o[b, sl, :] = keep_h * v["st"][b, sl, :] + outer[h * 64 : (h + 1) * 64]
        return 0

    lax.fori_loop(0, 8, st_step, 0)
    for d in range(1, 4):
        got(WM.at[(z + 4 - d) % 4], SEM_W + d - 1)

    def m_got(k, _):
        q = lax.rem(p_own + 1 + k, 16)
        got(M.at[q // 4, q % 4], SEM_M + q)
        return 0

    lax.fori_loop(0, 15, m_got, 0)
    part = dot(M[...].reshape(128, 2048), WM[...].reshape(128, 2048), NT)
    SQ[...] = part.reshape(16, 8, 128).astype(BF)
    mine = c * 16 + p_own

    def q_send(k, _):
        q = lax.rem(p_own + 1 + k, 16)
        send(SQ.at[q], R2.at[mine], SEM_Q + q * 2 + c, SEM_Q + mine, (z * 16 + q, c)).start()
        send(SQ.at[q], R2.at[mine], SEM_Q + q * 2 + oc, SEM_Q + mine, (z * 16 + q, oc)).start()
        return 0

    send(SQ.at[p_own], R2.at[mine], SEM_Q + p_own * 2 + oc, SEM_Q + mine, (e, oc)).start()
    lax.fori_loop(0, 15, q_send, 0)

    def q_sent(k, _):
        q = lax.rem(p_own + 1 + k, 16)
        sent(SQ.at[q], SEM_Q + q * 2)
        sent(SQ.at[q], SEM_Q + q * 2 + 1)
        return 0

    pending.append(lambda: lax.fori_loop(0, 15, q_sent, 0))
    pending.append(lambda: sent(SQ.at[p_own], SEM_Q + p_own * 2 + oc))
    R2[mine] = SQ[p_own]

    def q_got(k, _):
        q = lax.rem(p_own + 1 + k, 16)
        got(R2.at[q], SEM_Q + q)
        got(R2.at[16 + q], SEM_Q + 16 + q)
        return 0

    got(R2.at[oc * 16 + p_own], SEM_Q + oc * 16 + p_own)
    lax.fori_loop(0, 15, q_got, 0)
    tiles = [None] * 16
    for yy in range(4):
        a = [
            (R2[yy * 4 + xx].astype(F32) + R2[16 + yy * 4 + xx].astype(F32)).astype(BF).astype(F32)
            for xx in range(4)
        ]
        for zz in range(4):
            moved = [
                a[xx] if xx == zz else pltpu.roll(a[xx], (32 * (xx - zz)) % 128, 1)
                for xx in range(4)
            ]
            tiles[zz * 4 + yy] = lane_groups(moved, lane8)
    mixed_out = jnp.concatenate(tiles, axis=1)
    loads["g2"].wait()
    stream = (tok + mixed_out).astype(BF).astype(F32)
    ffn = rms(stream, v["g2"][...]).astype(BF)
    ff32 = ffn.astype(F32)

    half = jnp.where(c == 0, ff32[:, :HALF], ff32[:, HALF:])
    stacked = jnp.concatenate([half[:, j * 128 : (j + 1) * 128] for j in range(8)], axis=0)
    FF[...] = jnp.concatenate([stacked, jnp.zeros((64, 128), F32)], axis=0).astype(BF)
    SD[...] = dot(DM[...], FF[...]).reshape(64, 16, 128).astype(BF)

    def x_send(k, _):
        q = lax.rem(e + 1 + k, 64)
        send(SD.at[q], RX.at[c, e], SEM_X + q, SEM_X + e, (q, c)).start()
        return 0

    lax.fori_loop(0, 63, x_send, 0)

    def x_sent(k, _):
        q = lax.rem(e + 1 + k, 64)
        sent(SD.at[q], SEM_X + q)
        return 0

    pending.append(lambda: lax.fori_loop(0, 63, x_sent, 0))
    RX[c, e] = SD[e]

    for n in ("cg", "cu", "cd"):
        loads[n].wait()
    sh = (silu(dot(ffn, v["cg"][...])) * dot(ffn, v["cu"][...])).astype(BF)
    shared = dot(sh, v["cd"][...]).astype(BF)
    SHS[...] = shared
    send(SHS, SHR, SEM_SH, SEM_SH, (e, oc)).start()
    pending.append(lambda: sent(SHS, SEM_SH))
    for n in ("rg", "ru", "rd"):
        loads[n].wait()

    def x_got(k, _):
        q = lax.rem(e + 1 + k, 64)
        got(RX.at[c, q], SEM_X + q)
        return 0

    lax.fori_loop(0, 63, x_got, 0)
    send(RX.at[c], RX.at[c], SEM_FX, SEM_FX, (e, oc)).start()
    pending.append(lambda: sent(RX.at[c], SEM_FX))
    got(RX.at[oc], SEM_FX)
    lhs = []
    for h in range(2):
        XF[...] = RX[h].astype(F32).reshape(1024, 128)
        for j in range(8):
            lhs.append(XF[pl.ds(j, 128, stride=8), :].astype(BF))
    rows = jnp.concatenate(lhs, axis=1)
    hid = (silu(dot(rows, v["rg"][...])) * dot(rows, v["ru"][...])).astype(BF)
    theirs = pl.ds(pl.multiple_of(oc * HALF, HALF), HALF)
    ours = pl.ds(pl.multiple_of(c * HALF, HALF), HALF)
    YS[...] = dot(hid, v["rd"][:, theirs]).astype(BF)
    send(YS, YR, SEM_YE, SEM_YE, (e, oc)).start()
    pending.append(lambda: sent(YS, SEM_YE))
    part_y = dot(hid, v["rd"][:, ours]).astype(BF).astype(F32)
    got(YR, SEM_YE)
    total_y = part_y + YR[...].astype(F32)
    for j in range(8):
        XF[pl.ds(j, 128, stride=8), :] = total_y[:, j * 128 : (j + 1) * 128]
    SY[...] = XF[...].reshape(64, 16, 128).astype(BF)

    def y_send(k, _):
        q = lax.rem(e + 1 + k, 64)
        send(SY.at[q], RY.at[e], SEM_Y + q, SEM_Y + e, (q, c)).start()
        return 0

    lax.fori_loop(0, 63, y_send, 0)

    def y_sent(k, _):
        q = lax.rem(e + 1 + k, 64)
        sent(SY.at[q], SEM_Y + q)
        return 0

    pending.append(lambda: lax.fori_loop(0, 63, y_sent, 0))
    RY[e] = SY[e]
    got(SHR, SEM_SH)
    resid = stream + (shared.astype(F32) + SHR[...].astype(F32))
    resid_half = jnp.where(c == 0, resid[:, :HALF], resid[:, HALF:])

    def y_got(k, _):
        q = lax.rem(e + 1 + k, 64)
        got(RY.at[q], SEM_Y + q)
        return 0

    lax.fori_loop(0, 63, y_got, 0)
    both = dot(CM[...], RY[...].reshape(1024, 128))
    comb = both[0:64] + both[64:128]
    routed = jnp.concatenate([comb[j * 8 : (j + 1) * 8] for j in range(8)], axis=1)
    res = (resid_half + routed).astype(BF)
    RES[...] = res
    send(RES, RESR, SEM_RF, SEM_RF, (e, oc)).start()
    pending.append(lambda: sent(RES, SEM_RF))
    res_o[:, ours] = res
    got(RESR, SEM_RF)
    res_o[:, theirs] = RESR[...]
    finish()


def store_kernel(*refs):
    n = len(refs) // 2
    sem = refs[-1]
    copies = []
    for k in range(n):
        src, dst = refs[k], refs[n + k]
        if k == 1:
            copies += [(src.at[b], dst.at[b]) for b in range(8)]
        else:
            copies.append((src, dst))
    started = [pltpu.make_async_copy(a, b, sem.at[k]) for k, (a, b) in enumerate(copies)]
    for w in started:
        w.start()
    for w in started:
        w.wait()


def shards(
    tokens,
    mixer_norm_gain,
    gate_projection_weight,
    value_projection_weight,
    input_projection_weight,
    output_projection_weight,
    step_projection_weight,
    head_step_bias,
    head_decay_rate,
    extra_log_decay,
    value_taps,
    input_taps,
    output_taps,
    prior_values,
    prior_input_maps,
    prior_output_maps,
    head_skip_gain,
    group_norm_gain,
    mixer_output_weight,
    recurrent_state,
    expert_norm_gain,
    routes,
    chosen_expert_weight,
    routed_gate_weight,
    routed_up_weight,
    routed_down_weight,
    common_gate_weight,
    common_up_weight,
    common_down_weight,
):
    pv, pi, po = (
        jnp.transpose(a, (1, 0, 2)) for a in (prior_values, prior_input_maps, prior_output_maps)
    )
    state = recurrent_state.reshape(8, 2048, 128)
    vals = dict(
        tok=tokens,
        g1=mixer_norm_gain[None],
        wi=input_projection_weight,
        wo=output_projection_weight,
        wst=step_projection_weight.T,
        sb=head_step_bias[None],
        dr=head_decay_rate[None],
        eld=extra_log_decay,
        vt=value_taps,
        it=input_taps,
        ot=output_taps,
        pv=pv,
        pi=pi,
        po=po,
        hs=head_skip_gain[None],
        gg=group_norm_gain[None],
        g2=expert_norm_gain[None],
        routes=routes,
        cw=chosen_expert_weight,
        rg=routed_gate_weight[0],
        ru=routed_up_weight[0],
        rd=routed_down_weight[0],
        cg=common_gate_weight,
        cu=common_up_weight,
        cd=common_down_weight,
        st=state,
    )
    ins = [vals[n] for n in LOADED] + [
        jnp.transpose(gate_projection_weight, (1, 2, 0))[0],
        jnp.transpose(value_projection_weight, (1, 2, 0))[0],
        mixer_output_weight.T,
    ]
    vm = pltpu.VMEM
    scratch = [vm(vals[n].shape, vals[n].dtype) for n in LOADED] + [
        vm((2, 4, 4, 4, 8, HALF), BF),
        vm((4, 32, 2048), BF),
        vm((4, 32, 2048), BF),
        vm((64, 8, 128), BF),
        vm((64, 8, 128), BF),
        vm((4, 4, 8, 2048), BF),
        vm((16, 8, 128), BF),
        vm((32, 8, 128), BF),
        vm((64, 16, 128), BF),
        vm((2, 64, 16, 128), BF),
        vm((1024, 128), F32),
        vm((128, HALF), BF),
        vm((128, HALF), BF),
        vm((64, 16, 128), BF),
        vm((64, 16, 128), BF),
        vm((8, 2048), BF),
        vm((8, 2048), BF),
        vm((8, HALF), BF),
        vm((8, HALF), BF),
        vm((1024, 128), BF),
        vm((128, 1024), BF),
        vm((8, 2048), F32),
        vm((16, 512), BF),
        vm((128, 128), BF),
        vm((8, 512), F32),
        vm((8, 32, 128), F32),
        vm((2048, 128), BF),
        pltpu.SemaphoreType.DMA((len(LOADED) + 5,)),
        pltpu.SemaphoreType.DMA((SEM_COUNT,)),
        pltpu.SemaphoreType.DMA((SEM_COUNT,)),
    ]
    shapes = [
        ((8, 2048), BF),
        ((8, 2048, 128), F32),
        ((3, 8, 2048), BF),
        ((3, 8, 512), BF),
        ((3, 8, 512), BF),
    ]
    held = pl.pallas_call(
        layer_kernel,
        out_shape=[pltpu.VMEM(a, t) for a, t in shapes],
        in_specs=[pl.BlockSpec(memory_space=pltpu.HBM)] * len(ins),
        out_specs=[pl.BlockSpec(memory_space=pltpu.VMEM)] * 5,
        scratch_shapes=scratch,
        compiler_params=pltpu.CompilerParams(
            collective_id=0, has_side_effects=True, vmem_limit_bytes=50 * 2**20
        ),
    )(*ins)
    result, state_next, nv, ni, no = pl.pallas_call(
        store_kernel,
        out_shape=[jax.ShapeDtypeStruct(a, t) for a, t in shapes],
        in_specs=[pl.BlockSpec(memory_space=pl.ANY)] * 5,
        out_specs=[pl.BlockSpec(memory_space=pltpu.HBM)] * 5,
        scratch_shapes=[pltpu.SemaphoreType.DMA((12,))],
        compiler_params=pltpu.CompilerParams(vmem_limit_bytes=2**20),
    )(*held)
    return (
        result,
        state_next.reshape(8, 32, 64, 128),
        jnp.transpose(nv, (1, 0, 2)),
        jnp.transpose(ni, (1, 0, 2)),
        jnp.transpose(no, (1, 0, 2)),
    )


def solution(mesh):
    return jax.shard_map(
        shards,
        mesh=mesh,
        in_specs=(
            P("ep", None),
            P(),
            P(None, "tp", "ep"),
            P(None, "tp", "ep"),
            P(None, "tp"),
            P(None, "tp"),
            P(None, "tp"),
            P("tp"),
            P("tp"),
            P("ep", "tp"),
            P(None, "tp"),
            P(None, "tp"),
            P(None, "tp"),
            P("ep", None, "tp"),
            P("ep", None, "tp"),
            P("ep", None, "tp"),
            P("tp"),
            P("tp"),
            P("tp", "ep"),
            P("ep", "tp", None, None),
            P(),
            P("ep", None),
            P("ep", None),
            P("ep", None, "tp"),
            P("ep", None, "tp"),
            P("ep", "tp", None),
            P(None, "tp"),
            P(None, "tp"),
            P("tp", None),
        ),
        out_specs=(
            P("ep", None),
            P("ep", "tp", None, None),
            P("ep", None, "tp"),
            P("ep", None, "tp"),
            P("ep", None, "tp"),
        ),
        check_vma=False,
    )
```

```python
import functools

import jax
import jax.numpy as jnp
from jax import lax
from jax.experimental import pallas as pl
from jax.experimental.pallas import tpu as pltpu
from jax.sharding import PartitionSpec as P

MESH = pl.DeviceIdType.MESH
EPSILON = 1e-06
BF, F32 = jnp.bfloat16, jnp.float32
NT = (((1,), (1,)), ((), ()))
TN = (((0,), (0,)), ((), ()))
HALF = 1024
PIECES = ((0, 256), (256, 384), (640, 384))

SEM_A = 0
SEM_B = SEM_A + 48
SEM_F = SEM_B + 18
SEM_P = SEM_F + 12
SEM_W = SEM_P + 64
SEM_M = SEM_W + 3
SEM_Q = SEM_M + 16
SEM_X = SEM_Q + 32
SEM_Y = SEM_X + 64
SEM_FX = SEM_Y + 64
SEM_SH = SEM_FX + 1
SEM_YE = SEM_SH + 1
SEM_RF = SEM_YE + 1
SEM_COUNT = SEM_RF + 1

def hops(d):
    return sum(min(k, 4 - k) for k in d)


FAR = sorted(
    [(i // 16, i // 4 % 4, i % 4) for i in range(1, 64)], key=hops, reverse=True
)
FAR_PLANE = sorted([(i // 4, i % 4) for i in range(1, 16)], key=hops, reverse=True)

LOADED = (
    "tok", "g1", "wi", "wo", "wst", "sb", "dr", "eld", "vt", "it", "ot", "pv", "pi", "po", "hs",
    "gg", "g2", "routes", "cw", "rg", "ru", "rd", "cg", "cu", "cd", "st",
)


def silu(x):
    return x * (1.0 / (1.0 + jnp.exp(-x)))


def rms(x, gain):
    return x * lax.rsqrt(jnp.mean(x * x, axis=-1, keepdims=True) + EPSILON) * gain


def split_bf(x):
    hi = x.astype(BF)
    return hi, (x - hi.astype(F32)).astype(BF)


def dot(a, b, dims=(((1,), (0,)), ((), ()))):
    return lax.dot_general(a, b, dims, preferred_element_type=F32)


def lane_groups(pieces, lane):
    return jnp.where(
        lane < 32,
        pieces[0],
        jnp.where(lane < 64, pieces[1], jnp.where(lane < 96, pieces[2], pieces[3])),
    )


def layer_kernel(*refs):
    hbm = dict(zip(LOADED + ("gt", "vtp", "wmt"), refs[:29]))
    res_o, st_o, nv_o, ni_o, no_o = refs[29:34]
    v = dict(zip(LOADED, refs[34:60]))
    (
        X, WGV, WM, SP, R1, M, SQ, R2, SD, RX, XF, YS, YR, SY, RY, SHS, SHR, RES, RESR, DM, CM, QR,
        CC, FF, BV, DV, UT, ld, ss, rs,
    ) = refs[60:]

    e = lax.axis_index("ep")
    c = lax.axis_index("tp")
    oc = 1 - c
    z, y, x = e // 16, (e // 4) % 4, e % 4
    own = (z, y, x)

    def ep_of(zz, yy, xx):
        return zz * 16 + yy * 4 + xx

    def send(src, dst, so, ro, dev):
        return pltpu.make_async_remote_copy(
            src_ref=src, dst_ref=dst, send_sem=ss.at[so], recv_sem=rs.at[ro],
            device_id=dev, device_id_type=MESH,
        )

    def got(dst, ro):
        send(dst, dst, ro, ro, (e, oc)).wait_recv()

    def sent(src, so):
        send(src, src, so, so, (e, oc)).wait_send()

    pending = []

    def finish():
        for f in pending:
            f()
        pending.clear()

    loads = {}
    for k, n in enumerate(LOADED):
        loads[n] = pltpu.make_async_copy(hbm[n], v[n], ld.at[k])
    base = len(LOADED)
    gcopy = pltpu.make_async_copy(hbm["gt"], WGV.at[x], ld.at[base])
    vcopies = [
        pltpu.make_async_copy(hbm["vtp"], WGV.at[(x + 1 + j) % 4], ld.at[base + 1 + j])
        for j in range(3)
    ]
    wcopy = pltpu.make_async_copy(hbm["wmt"], WM.at[z], ld.at[base + 4])
    loads["tok"].start()
    loads["g1"].start()
    wcopy.start()
    loads["wst"].start()
    for n in ("wi", "wo", "sb", "dr", "eld", "vt", "it", "ot", "pv", "pi", "po", "hs", "gg", "g2", "routes", "cw"):
        loads[n].start()
    gcopy.start()
    for w in vcopies:
        w.start()
    for n in ("st", "cg", "cu", "cd", "rg", "ru", "rd"):
        loads[n].start()

    bar = pltpu.get_barrier_semaphore()
    pl.semaphore_signal(bar, inc=1, device_id=(e, oc), device_id_type=MESH)

    zs, ys, xs = ([(w + d) % 4 for d in range(4)] for w in own)

    def peer(d):
        return zs[d[0]] * 16 + ys[d[1]] * 4 + xs[d[2]]

    p_own = y * 4 + x

    def plane_peer(d):
        return ys[d[0]] * 4 + xs[d[1]]

    greeted = [d for d in FAR if 0 in d]
    for d in greeted:
        pl.semaphore_signal(bar, inc=1, device_id=(peer(d), c), device_id_type=MESH)

    loads["tok"].wait()
    loads["g1"].wait()
    tok = v["tok"][...].astype(F32)
    normed = rms(tok, v["g1"][...]).astype(BF)
    nf = normed.astype(F32)
    X[c, z, y, x] = jnp.where(c == 0, nf[:, :HALF], nf[:, HALF:]).astype(BF)

    pl.semaphore_wait(bar, 1 + len(greeted))

    def coords(i, line, p):
        a, b = p // 4, p % 4
        return ((line, a, b), (a, line, b), (a, b, line))[i]

    def plane_index(i):
        return (y * 4 + x, z * 4 + x, z * 4 + y)[i]

    def cols(i):
        return pl.ds(PIECES[i][0], PIECES[i][1])

    def own_piece(i):
        return X.at[c, z, y, x, :, cols(i)]

    def a_send(k, _):
        for i in range(3):
            p = plane_index(i)
            q = lax.rem(p + 1 + k, 16)
            dev = (ep_of(*coords(i, own[i], q)), c)
            send(own_piece(i), own_piece(i), SEM_A + i * 16 + q, SEM_A + i * 16 + p, dev).start()
        return 0

    lax.fori_loop(0, 15, a_send, 0)

    def a_sent(k, _):
        for i in range(3):
            q = lax.rem(plane_index(i) + 1 + k, 16)
            sent(own_piece(i), SEM_A + i * 16 + q)
        return 0

    pending.append(lambda: lax.fori_loop(0, 15, a_sent, 0))

    wcopy.wait()
    for d in range(1, 4):
        dev = (ep_of((z + d) % 4, y, x), c)
        send(WM.at[z], WM.at[z], SEM_W + d - 1, SEM_W + d - 1, dev).start()
        pending.append(lambda d=d: sent(WM.at[z], SEM_W + d - 1))

    for n in ("wi", "wo", "wst", "sb", "dr", "eld", "it", "ot", "pi", "po"):
        loads[n].wait()
    in_rows = dot(normed, v["wi"][...]).astype(BF)
    out_rows = dot(normed, v["wo"][...]).astype(BF)
    step_raw = dot(normed, v["wst"][...], NT)

    def conv(prior, fresh, taps):
        t = taps[...]
        total = fresh * t[3:4]
        for j in range(3):
            total = total + prior[j].astype(F32) * t[j : j + 1]
        return silu(total)

    b_conv = conv(v["pi"], in_rows.astype(F32), v["it"])
    c_conv = conv(v["po"], out_rows.astype(F32), v["ot"])
    BV[...] = b_conv
    pre = step_raw + v["sb"][...]
    dt = jnp.maximum(pre, 0.0) + jnp.log(1.0 + jnp.exp(-jnp.abs(pre)))
    dec = jnp.exp(-dt * v["dr"][...] + v["eld"][...])
    c_hi, c_lo = split_bf(c_conv)
    CC[...] = jnp.concatenate([c_hi.astype(F32), c_lo.astype(F32)], axis=0).astype(BF)

    def plane(i, line, h=None):
        part = slice(None) if h is None else pl.ds(2 * h, 2)
        if i == 0:
            return X.at[c, line, part, :, :, cols(i)]
        if i == 1:
            return X.at[c, part, line, :, :, cols(i)]
        return X.at[c, part, :, line, :, cols(i)]

    def line_peer(i, d):
        there = list(own)
        there[i] = (own[i] + d) % 4
        return (ep_of(*there), c)

    def line_send(i, line, h, d, k):
        src = plane(i, line, h)
        k = SEM_B + i * 6 + k
        send(src, src, k, k, line_peer(i, d)).start()
        pending.append(lambda: sent(plane(i, line, h), k))

    def hand_over(i, d):
        line = (own[i] + d) % 4
        k = SEM_F + i * 4 + d
        send(plane(i, line), plane(i, line), k, k, (e, oc)).start()
        pending.append(lambda: sent(plane(i, line), k))

    def a_got(k, _):
        for i in range(3):
            q = lax.rem(plane_index(i) + 1 + k, 16)
            zz, yy, xx = coords(i, own[i], q)
            got(X.at[c, zz, yy, xx, :, cols(i)], SEM_A + i * 16 + q)
        return 0

    lax.fori_loop(0, 15, a_got, 0)
    for k, (h, d) in enumerate(((0, 1), (1, 3), (1, 1), (0, 3))):
        for i in range(3):
            line_send(i, own[i], h, d, k)
    for i in range(3):
        hand_over(i, 0)

    loads["st"].wait()
    row = lax.broadcasted_iota(jnp.int32, (8, 512), 0)
    QR[...] = jnp.zeros((8, 2048), F32)

    def q_step(b, _):
        for g in range(4):
            s = v["st"][b, g * 512 : (g + 1) * 512, :].astype(BF)
            r = dot(CC[:, g * 128 : (g + 1) * 128], s, NT)
            sl = pl.ds(g * 512, 512)
            QR[:, sl] = jnp.where(row == b, r[0:8] + r[8:16], QR[:, sl])
        return 0

    lax.fori_loop(0, 8, q_step, 0)

    d1 = dec.astype(BF)
    d2 = (dec - d1.astype(F32)).astype(BF)
    seq = lax.broadcasted_iota(jnp.int32, (8, 1024), 1) // 128
    ones = (seq == lax.broadcasted_iota(jnp.int32, (8, 1024), 0)).astype(BF)
    spread_dec = dot(d1, ones, TN) + dot(d2, ones, TN)
    for b in range(8):
        DV[b] = spread_dec[:, b * 128 : (b + 1) * 128]

    loads["hs"].wait()
    spread = (
        lax.broadcasted_iota(jnp.int32, (32, 2048), 1) // 64
        == lax.broadcasted_iota(jnp.int32, (32, 2048), 0)
    ).astype(BF)
    heads = jnp.concatenate([dt, dec, jnp.broadcast_to(v["hs"][...], (8, 32))], axis=0)
    h1 = heads.astype(BF)
    r1 = heads - h1.astype(F32)
    h2 = r1.astype(BF)
    h3 = (r1 - h2.astype(F32)).astype(BF)
    wide = dot(h1, spread) + dot(h2, spread) + dot(h3, spread)
    dt_w, dec_w, skip_w = wide[0:8], wide[8:16], wide[16:24]
    bc = b_conv * c_conv
    bc_w = jnp.concatenate(
        [
            jnp.broadcast_to(
                jnp.sum(bc[:, g * 128 : (g + 1) * 128], axis=1, keepdims=True), (8, 512)
            )
            for g in range(4)
        ],
        axis=1,
    )
    kept = dec_w * QR[...]
    v_gain = dt_w * bc_w + skip_w

    for i in range(3):
        before, after = (own[i] + 3) % 4, (own[i] + 1) % 4
        got(plane(i, before, 0), SEM_B + i * 6)
        line_send(i, before, 0, 1, 4)
        got(plane(i, after, 1), SEM_B + i * 6 + 1)
        line_send(i, after, 1, 3, 5)
    for i in range(3):
        before, after = (own[i] + 3) % 4, (own[i] + 1) % 4
        got(plane(i, before, 1), SEM_B + i * 6 + 2)
        hand_over(i, 3)
        got(plane(i, after, 0), SEM_B + i * 6 + 3)
        hand_over(i, 1)
    for i in range(3):
        across = (own[i] + 2) % 4
        got(plane(i, across, 0), SEM_B + i * 6 + 4)
        got(plane(i, across, 1), SEM_B + i * 6 + 5)
        hand_over(i, 2)
    gcopy.wait()
    for w in vcopies:
        w.wait()
    proj = jnp.zeros((512, 128), F32)
    for i in range(3):
        for d in range(4):
            line = (own[i] + d) % 4
            view = X.at[oc]
            if i == 0:
                view = view.at[line, :, :, :, cols(i)]
            elif i == 1:
                view = view.at[:, line, :, :, cols(i)]
            else:
                view = view.at[:, :, line, :, cols(i)]
            got(view, SEM_F + i * 4 + d)
        at, width = PIECES[i]
        for h in range(2):
            w = WGV[:, :, h * HALF + at : h * HALF + at + width].reshape(128, width)
            proj = proj + dot(X[h, :, :, :, :, at : at + width].reshape(512, width), w, NT)
    SP[...] = proj.reshape(64, 8, 128).astype(BF)

    for d in FAR:
        q = peer(d)
        send(SP.at[q], R1.at[e], SEM_P + q, SEM_P + e, (q, c)).start()

    def p_sent(k, _):
        q = lax.rem(e + 1 + k, 64)
        sent(SP.at[q], SEM_P + q)
        return 0

    pending.append(lambda: lax.fori_loop(0, 63, p_sent, 0))
    R1[e] = SP[e]

    loads["routes"].wait()
    loads["cw"].wait()
    lane8 = lax.broadcasted_iota(jnp.int32, (8, 128), 1)
    hit = jnp.zeros((8, 128), F32)
    wgt = jnp.zeros((8, 128), F32)
    rt = v["routes"][...]
    cwv = v["cw"][...]
    for k in range(6):
        eq = lane8 == rt[:, k : k + 1]
        hit = hit + jnp.where(eq, 1.0, 0.0)
        wgt = wgt + jnp.where(eq, cwv[:, k : k + 1], 0.0)
    before = (
        lax.broadcasted_iota(jnp.int32, (8, 8), 0) > lax.broadcasted_iota(jnp.int32, (8, 8), 1)
    ).astype(BF)
    slot = dot(before, hit.astype(BF))
    s0 = jnp.where(slot < 0.5, 1.0, 0.0)
    w1 = wgt.astype(BF).astype(F32)
    w2 = wgt - w1
    rows6 = jnp.concatenate(
        [hit * s0, hit * (1 - s0), w1 * s0, w1 * (1 - s0), w2 * s0, w2 * (1 - s0)], axis=0
    ).astype(BF)
    place = (
        lax.broadcasted_iota(jnp.int32, (128, 1024), 1) // 16
        == lax.broadcasted_iota(jnp.int32, (128, 1024), 0)
    ).astype(BF)
    six = dot(rows6, place)
    lane_r = lax.broadcasted_iota(jnp.int32, (8, 1024), 1)
    first = (lane_r // 8) % 2 == 0
    hsel = jnp.where(first, six[0:8], six[8:16])
    w1s = jnp.where(first, six[16:24], six[24:32])
    w2s = jnp.where(first, six[32:40], six[40:48])
    tile = lane_r % 8
    zero = jnp.zeros((8, 1024), F32)

    def diag(a):
        return jnp.concatenate([jnp.where(tile == j, a, zero) for j in range(8)], axis=0)

    DM[...] = jnp.concatenate([diag(hsel), jnp.zeros((64, 1024), F32)], axis=0).T.astype(BF)
    CM[...] = jnp.concatenate([diag(w1s), diag(w2s)], axis=0).astype(BF)
    for n in ("vt", "pv", "gg"):
        loads[n].wait()

    for d in FAR[::-1]:
        q = peer(d)
        got(R1.at[q], SEM_P + q)

    gates, values = [], []
    for t in range(16):
        r = [R1[4 * t + j].astype(F32) for j in range(4)]
        gates.append(lane_groups(r, lane8))
        values.append(pltpu.roll(lane_groups([r[3], r[0], r[1], r[2]], lane8), 96, 1))
    gate = jnp.concatenate(gates, axis=1)
    value = jnp.concatenate(values, axis=1)
    value_rows = value.astype(BF)
    v_conv = conv(v["pv"], value, v["vt"])
    mixed = (kept + v_conv * v_gain) * silu(gate)
    normed_groups = []
    for g in range(4):
        m = mixed[:, g * 512 : (g + 1) * 512]
        normed_groups.append(m * lax.rsqrt(jnp.mean(m * m, axis=1, keepdims=True) + EPSILON))
    mixer_rows = jnp.concatenate(normed_groups, axis=1) * v["gg"][...]
    M[y, x] = mixer_rows.astype(BF)

    for d in FAR_PLANE:
        q = plane_peer(d)
        send(M.at[y, x], M.at[y, x], SEM_M + q, SEM_M + p_own, (z * 16 + q, c)).start()

    def m_sent(k, _):
        sent(M.at[y, x], SEM_M + lax.rem(p_own + 1 + k, 16))
        return 0

    pending.append(lambda: lax.fori_loop(0, 15, m_sent, 0))
    for new, old, fresh in ((nv_o, "pv", value_rows), (ni_o, "pi", in_rows), (no_o, "po", out_rows)):
        new[0] = v[old][1]
        new[1] = v[old][2]
        new[2] = fresh

    u = v_conv * dt_w
    u1 = u.astype(BF).astype(F32)
    pad = jnp.zeros((104, 2048), F32)
    UT[...] = jnp.concatenate([u1, u1, u - u1, pad], axis=0).T.astype(BF)

    def st_step(b, _):
        bv = BV[...]
        b1 = bv.astype(BF).astype(F32)
        keep = lax.broadcasted_iota(jnp.int32, (8, 512), 0) == b
        zero = jnp.zeros((8, 512), F32)
        k1, k2 = jnp.where(keep, b1, zero), jnp.where(keep, bv - b1, zero)
        rhs = jnp.concatenate([k1, k2, k1, jnp.zeros((104, 512), F32)], axis=0).astype(BF)
        for g in range(4):
            outer = dot(UT[g * 512 : (g + 1) * 512, :], rhs[:, g * 128 : (g + 1) * 128])
            for h in range(8):
                sl = pl.ds(g * 512 + h * 64, 64)
                keep_h = DV[b, pl.ds(g * 8 + h, 1), :]
                st_o[b, sl, :] = keep_h * v["st"][b, sl, :] + outer[h * 64 : (h + 1) * 64]
        return 0

    lax.fori_loop(0, 8, st_step, 0)
    finish()
    for d in range(1, 4):
        got(WM.at[(z + 4 - d) % 4], SEM_W + d - 1)

    def m_got(k, _):
        q = lax.rem(p_own + 1 + k, 16)
        got(M.at[q // 4, q % 4], SEM_M + q)
        return 0

    lax.fori_loop(0, 15, m_got, 0)
    part = dot(M[...].reshape(128, 2048), WM[...].reshape(128, 2048), NT)
    SQ[...] = part.reshape(16, 8, 128).astype(BF)
    mine = c * 16 + p_own

    for d in FAR_PLANE:
        q = plane_peer(d)
        send(SQ.at[q], R2.at[mine], SEM_Q + q * 2 + oc, SEM_Q + mine, (z * 16 + q, oc)).start()
        send(SQ.at[q], R2.at[mine], SEM_Q + q * 2 + c, SEM_Q + mine, (z * 16 + q, c)).start()
    send(SQ.at[p_own], R2.at[mine], SEM_Q + p_own * 2 + oc, SEM_Q + mine, (e, oc)).start()

    def q_sent(k, _):
        q = lax.rem(p_own + 1 + k, 16)
        sent(SQ.at[q], SEM_Q + q * 2)
        sent(SQ.at[q], SEM_Q + q * 2 + 1)
        return 0

    pending.append(lambda: lax.fori_loop(0, 15, q_sent, 0))
    pending.append(lambda: sent(SQ.at[p_own], SEM_Q + p_own * 2 + oc))
    R2[mine] = SQ[p_own]

    def q_got(k, _):
        q = lax.rem(p_own + 1 + k, 16)
        got(R2.at[q], SEM_Q + q)
        got(R2.at[16 + q], SEM_Q + 16 + q)
        return 0

    got(R2.at[oc * 16 + p_own], SEM_Q + oc * 16 + p_own)
    lax.fori_loop(0, 15, q_got, 0)
    tiles = [None] * 16
    for yy in range(4):
        a = [
            (R2[yy * 4 + xx].astype(F32) + R2[16 + yy * 4 + xx].astype(F32)).astype(BF).astype(F32)
            for xx in range(4)
        ]
        for zz in range(4):
            moved = [
                a[xx] if xx == zz else pltpu.roll(a[xx], (32 * (xx - zz)) % 128, 1)
                for xx in range(4)
            ]
            tiles[zz * 4 + yy] = lane_groups(moved, lane8)
    mixed_out = jnp.concatenate(tiles, axis=1)
    loads["g2"].wait()
    stream = (tok + mixed_out).astype(BF).astype(F32)
    ffn = rms(stream, v["g2"][...]).astype(BF)
    ff32 = ffn.astype(F32)

    half = jnp.where(c == 0, ff32[:, :HALF], ff32[:, HALF:])
    stacked = jnp.concatenate([half[:, j * 128 : (j + 1) * 128] for j in range(8)], axis=0)
    FF[...] = jnp.concatenate([stacked, jnp.zeros((64, 128), F32)], axis=0).astype(BF)
    SD[...] = dot(DM[...], FF[...]).reshape(64, 16, 128).astype(BF)

    for d in FAR:
        q = peer(d)
        send(SD.at[q], RX.at[c, e], SEM_X + q, SEM_X + e, (q, c)).start()

    def x_sent(k, _):
        q = lax.rem(e + 1 + k, 64)
        sent(SD.at[q], SEM_X + q)
        return 0

    pending.append(lambda: lax.fori_loop(0, 63, x_sent, 0))
    RX[c, e] = SD[e]

    for n in ("cg", "cu", "cd"):
        loads[n].wait()
    sh = (silu(dot(ffn, v["cg"][...])) * dot(ffn, v["cu"][...])).astype(BF)
    shared = dot(sh, v["cd"][...]).astype(BF)
    SHS[...] = shared
    send(SHS, SHR, SEM_SH, SEM_SH, (e, oc)).start()
    pending.append(lambda: sent(SHS, SEM_SH))
    for n in ("rg", "ru", "rd"):
        loads[n].wait()

    for d in FAR[::-1]:
        q = peer(d)
        got(RX.at[c, q], SEM_X + q)
    send(RX.at[c], RX.at[c], SEM_FX, SEM_FX, (e, oc)).start()
    pending.append(lambda: sent(RX.at[c], SEM_FX))
    got(RX.at[oc], SEM_FX)
    lhs = []
    for h in range(2):
        XF[...] = RX[h].astype(F32).reshape(1024, 128)
        for j in range(8):
            lhs.append(XF[pl.ds(j, 128, stride=8), :].astype(BF))
    rows = jnp.concatenate(lhs, axis=1)
    hid = (silu(dot(rows, v["rg"][...])) * dot(rows, v["ru"][...])).astype(BF)
    theirs = pl.ds(pl.multiple_of(oc * HALF, HALF), HALF)
    ours = pl.ds(pl.multiple_of(c * HALF, HALF), HALF)
    YS[...] = dot(hid, v["rd"][:, theirs]).astype(BF)
    send(YS, YR, SEM_YE, SEM_YE, (e, oc)).start()
    pending.append(lambda: sent(YS, SEM_YE))
    part_y = dot(hid, v["rd"][:, ours]).astype(BF).astype(F32)
    got(YR, SEM_YE)
    total_y = part_y + YR[...].astype(F32)
    for j in range(8):
        XF[pl.ds(j, 128, stride=8), :] = total_y[:, j * 128 : (j + 1) * 128]
    SY[...] = XF[...].reshape(64, 16, 128).astype(BF)

    for d in FAR:
        q = peer(d)
        send(SY.at[q], RY.at[e], SEM_Y + q, SEM_Y + e, (q, c)).start()

    def y_sent(k, _):
        q = lax.rem(e + 1 + k, 64)
        sent(SY.at[q], SEM_Y + q)
        return 0

    pending.append(lambda: lax.fori_loop(0, 63, y_sent, 0))
    RY[e] = SY[e]
    got(SHR, SEM_SH)
    resid = stream + (shared.astype(F32) + SHR[...].astype(F32))
    resid_half = jnp.where(c == 0, resid[:, :HALF], resid[:, HALF:])

    while len(pending) > 1:
        pending.pop(0)()
    for d in FAR[::-1]:
        q = peer(d)
        got(RY.at[q], SEM_Y + q)
    both = dot(CM[...], RY[...].reshape(1024, 128))
    comb = both[0:64] + both[64:128]
    routed = jnp.concatenate([comb[j * 8 : (j + 1) * 8] for j in range(8)], axis=1)
    res = (resid_half + routed).astype(BF)
    RES[...] = res
    send(RES, RESR, SEM_RF, SEM_RF, (e, oc)).start()
    pending.append(lambda: sent(RES, SEM_RF))
    res_o[:, ours] = res
    got(RESR, SEM_RF)
    res_o[:, theirs] = RESR[...]
    finish()


def store_kernel(*refs):
    n = len(refs) // 2
    sem = refs[-1]
    copies = []
    for k in range(n):
        src, dst = refs[k], refs[n + k]
        if k == 1:
            copies += [(src.at[b], dst.at[b]) for b in range(8)]
        else:
            copies.append((src, dst))
    started = [pltpu.make_async_copy(a, b, sem.at[k]) for k, (a, b) in enumerate(copies)]
    for w in started:
        w.start()
    for w in started:
        w.wait()


def shards(
    tokens,
    mixer_norm_gain,
    gate_projection_weight,
    value_projection_weight,
    input_projection_weight,
    output_projection_weight,
    step_projection_weight,
    head_step_bias,
    head_decay_rate,
    extra_log_decay,
    value_taps,
    input_taps,
    output_taps,
    prior_values,
    prior_input_maps,
    prior_output_maps,
    head_skip_gain,
    group_norm_gain,
    mixer_output_weight,
    recurrent_state,
    expert_norm_gain,
    routes,
    chosen_expert_weight,
    routed_gate_weight,
    routed_up_weight,
    routed_down_weight,
    common_gate_weight,
    common_up_weight,
    common_down_weight,
):
    pv, pi, po = (
        jnp.transpose(a, (1, 0, 2)) for a in (prior_values, prior_input_maps, prior_output_maps)
    )
    state = recurrent_state.reshape(8, 2048, 128)
    vals = dict(
        tok=tokens,
        g1=mixer_norm_gain[None],
        wi=input_projection_weight,
        wo=output_projection_weight,
        wst=step_projection_weight.T,
        sb=head_step_bias[None],
        dr=head_decay_rate[None],
        eld=extra_log_decay,
        vt=value_taps,
        it=input_taps,
        ot=output_taps,
        pv=pv,
        pi=pi,
        po=po,
        hs=head_skip_gain[None],
        gg=group_norm_gain[None],
        g2=expert_norm_gain[None],
        routes=routes,
        cw=chosen_expert_weight,
        rg=routed_gate_weight[0],
        ru=routed_up_weight[0],
        rd=routed_down_weight[0],
        cg=common_gate_weight,
        cu=common_up_weight,
        cd=common_down_weight,
        st=state,
    )
    ins = [vals[n] for n in LOADED] + [
        jnp.transpose(gate_projection_weight, (1, 2, 0))[0],
        jnp.transpose(value_projection_weight, (1, 2, 0))[0],
        mixer_output_weight.T,
    ]
    vm = pltpu.VMEM
    scratch = [vm(vals[n].shape, vals[n].dtype) for n in LOADED] + [
        vm((2, 4, 4, 4, 8, HALF), BF),
        vm((4, 32, 2048), BF),
        vm((4, 32, 2048), BF),
        vm((64, 8, 128), BF),
        vm((64, 8, 128), BF),
        vm((4, 4, 8, 2048), BF),
        vm((16, 8, 128), BF),
        vm((32, 8, 128), BF),
        vm((64, 16, 128), BF),
        vm((2, 64, 16, 128), BF),
        vm((1024, 128), F32),
        vm((128, HALF), BF),
        vm((128, HALF), BF),
        vm((64, 16, 128), BF),
        vm((64, 16, 128), BF),
        vm((8, 2048), BF),
        vm((8, 2048), BF),
        vm((8, HALF), BF),
        vm((8, HALF), BF),
        vm((1024, 128), BF),
        vm((128, 1024), BF),
        vm((8, 2048), F32),
        vm((16, 512), BF),
        vm((128, 128), BF),
        vm((8, 512), F32),
        vm((8, 32, 128), F32),
        vm((2048, 128), BF),
        pltpu.SemaphoreType.DMA((len(LOADED) + 5,)),
        pltpu.SemaphoreType.DMA((SEM_COUNT,)),
        pltpu.SemaphoreType.DMA((SEM_COUNT,)),
    ]
    shapes = [
        ((8, 2048), BF),
        ((8, 2048, 128), F32),
        ((3, 8, 2048), BF),
        ((3, 8, 512), BF),
        ((3, 8, 512), BF),
    ]
    held = pl.pallas_call(
        layer_kernel,
        out_shape=[pltpu.VMEM(a, t) for a, t in shapes],
        in_specs=[pl.BlockSpec(memory_space=pltpu.HBM)] * len(ins),
        out_specs=[pl.BlockSpec(memory_space=pltpu.VMEM)] * 5,
        scratch_shapes=scratch,
        compiler_params=pltpu.CompilerParams(
            collective_id=0, has_side_effects=True, vmem_limit_bytes=50 * 2**20
        ),
    )(*ins)
    result, state_next, nv, ni, no = pl.pallas_call(
        store_kernel,
        out_shape=[jax.ShapeDtypeStruct(a, t) for a, t in shapes],
        in_specs=[pl.BlockSpec(memory_space=pl.ANY)] * 5,
        out_specs=[pl.BlockSpec(memory_space=pltpu.HBM)] * 5,
        scratch_shapes=[pltpu.SemaphoreType.DMA((12,))],
        compiler_params=pltpu.CompilerParams(vmem_limit_bytes=2**20),
    )(*held)
    return (
        result,
        state_next.reshape(8, 32, 64, 128),
        jnp.transpose(nv, (1, 0, 2)),
        jnp.transpose(ni, (1, 0, 2)),
        jnp.transpose(no, (1, 0, 2)),
    )


def solution(mesh):
    return jax.shard_map(
        shards,
        mesh=mesh,
        in_specs=(
            P("ep", None),
            P(),
            P(None, "tp", "ep"),
            P(None, "tp", "ep"),
            P(None, "tp"),
            P(None, "tp"),
            P(None, "tp"),
            P("tp"),
            P("tp"),
            P("ep", "tp"),
            P(None, "tp"),
            P(None, "tp"),
            P(None, "tp"),
            P("ep", None, "tp"),
            P("ep", None, "tp"),
            P("ep", None, "tp"),
            P("tp"),
            P("tp"),
            P("tp", "ep"),
            P("ep", "tp", None, None),
            P(),
            P("ep", None),
            P("ep", None),
            P("ep", None, "tp"),
            P("ep", None, "tp"),
            P("ep", "tp", None),
            P(None, "tp"),
            P(None, "tp"),
            P("tp", None),
        ),
        out_specs=(
            P("ep", None),
            P("ep", "tp", None, None),
            P("ep", None, "tp"),
            P("ep", None, "tp"),
            P("ep", None, "tp"),
        ),
        check_vma=False,
    )
```

```python
import functools

import jax
import jax.numpy as jnp
from jax import lax
from jax.experimental import pallas as pl
from jax.experimental.pallas import tpu as pltpu
from jax.sharding import PartitionSpec as P

MESH = pl.DeviceIdType.MESH
EPSILON = 1e-06
BF, F32 = jnp.bfloat16, jnp.float32
NT = (((1,), (1,)), ((), ()))
TN = (((0,), (0,)), ((), ()))
HALF = 1024
PIECES = ((0, 256), (256, 384), (640, 384))

SEM_A = 0
SEM_B = SEM_A + 48
SEM_F = SEM_B + 18
SEM_P = SEM_F + 12
SEM_W = SEM_P + 64
SEM_M = SEM_W + 16
SEM_Q = SEM_M + 4
SEM_X = SEM_Q + 8
SEM_Y = SEM_X + 64
SEM_FX = SEM_Y + 64
SEM_SH = SEM_FX + 4
SEM_YE = SEM_SH + 1
SEM_RF = SEM_YE + 1
SEM_COUNT = SEM_RF + 1

def hops(d):
    return sum(min(k, 4 - k) for k in d)


FAR = sorted(
    [(i // 16, i // 4 % 4, i % 4) for i in range(1, 64)], key=hops, reverse=True
)

LOADED = (
    "tok", "g1", "wi", "wo", "wst", "sb", "dr", "eld", "vt", "it", "ot", "pv", "pi", "po", "hs",
    "gg", "g2", "routes", "cw", "rg", "ru", "rd", "cg", "cu", "cd", "st",
)


def silu(x):
    return x * (1.0 / (1.0 + jnp.exp(-x)))


def rms(x, gain):
    return x * lax.rsqrt(jnp.mean(x * x, axis=-1, keepdims=True) + EPSILON) * gain


def split_bf(x):
    hi = x.astype(BF)
    return hi, (x - hi.astype(F32)).astype(BF)


def dot(a, b, dims=(((1,), (0,)), ((), ()))):
    return lax.dot_general(a, b, dims, preferred_element_type=F32)


def lane_groups(pieces, lane):
    return jnp.where(
        lane < 32,
        pieces[0],
        jnp.where(lane < 64, pieces[1], jnp.where(lane < 96, pieces[2], pieces[3])),
    )


def layer_kernel(*refs):
    hbm = dict(zip(LOADED + ("gt", "vtp", "wmt"), refs[:29]))
    res_o, st_o, nv_o, ni_o, no_o = refs[29:34]
    v = dict(zip(LOADED, refs[34:60]))
    (
        X, WGV, WM, SP, R1, M, SQ, R2, SD, RX, XF, YS, YR, SY, RY, SHS, SHR, RES, RESR, DM, CM, QR,
        CC, FF, BV, DV, UT, ld, ss, rs,
    ) = refs[60:]

    e = lax.axis_index("ep")
    c = lax.axis_index("tp")
    oc = 1 - c
    z, y, x = e // 16, (e // 4) % 4, e % 4
    own = (z, y, x)

    def ep_of(zz, yy, xx):
        return zz * 16 + yy * 4 + xx

    def send(src, dst, so, ro, dev):
        return pltpu.make_async_remote_copy(
            src_ref=src, dst_ref=dst, send_sem=ss.at[so], recv_sem=rs.at[ro],
            device_id=dev, device_id_type=MESH,
        )

    def got(dst, ro):
        send(dst, dst, ro, ro, (e, oc)).wait_recv()

    def sent(src, so):
        send(src, src, so, so, (e, oc)).wait_send()

    pending = []

    def finish():
        for f in pending:
            f()
        pending.clear()

    loads = {}
    for k, n in enumerate(LOADED):
        loads[n] = pltpu.make_async_copy(hbm[n], v[n], ld.at[k])
    base = len(LOADED)
    gcopy = pltpu.make_async_copy(hbm["gt"], WGV.at[x], ld.at[base])
    vcopies = [
        pltpu.make_async_copy(hbm["vtp"], WGV.at[(x + 1 + j) % 4], ld.at[base + 1 + j])
        for j in range(3)
    ]
    wcopy = pltpu.make_async_copy(hbm["wmt"], WM.at[z, y], ld.at[base + 4])
    loads["tok"].start()
    loads["g1"].start()
    wcopy.start()
    loads["wst"].start()
    for n in ("wi", "wo", "sb", "dr", "eld", "vt", "it", "ot", "pv", "pi", "po", "hs", "gg", "g2", "routes", "cw"):
        loads[n].start()
    gcopy.start()
    for w in vcopies:
        w.start()
    for n in ("st", "cg", "cu", "cd", "rg", "ru", "rd"):
        loads[n].start()

    bar = pltpu.get_barrier_semaphore()
    pl.semaphore_signal(bar, inc=1, device_id=(e, oc), device_id_type=MESH)

    zs, ys, xs = ([(w + d) % 4 for d in range(4)] for w in own)

    def peer(d):
        return zs[d[0]] * 16 + ys[d[1]] * 4 + xs[d[2]]

    greeted = [d for d in FAR if 0 in d]
    for d in greeted:
        pl.semaphore_signal(bar, inc=1, device_id=(peer(d), c), device_id_type=MESH)

    loads["tok"].wait()
    loads["g1"].wait()
    tok = v["tok"][...].astype(F32)
    normed = rms(tok, v["g1"][...]).astype(BF)
    nf = normed.astype(F32)
    X[c, z, y, x] = jnp.where(c == 0, nf[:, :HALF], nf[:, HALF:]).astype(BF)

    pl.semaphore_wait(bar, 1 + len(greeted))

    def coords(i, line, p):
        a, b = p // 4, p % 4
        return ((line, a, b), (a, line, b), (a, b, line))[i]

    def plane_index(i):
        return (y * 4 + x, z * 4 + x, z * 4 + y)[i]

    def cols(i):
        return pl.ds(PIECES[i][0], PIECES[i][1])

    def own_piece(i):
        return X.at[c, z, y, x, :, cols(i)]

    def a_send(k, _):
        for i in range(3):
            p = plane_index(i)
            q = lax.rem(p + 1 + k, 16)
            dev = (ep_of(*coords(i, own[i], q)), c)
            send(own_piece(i), own_piece(i), SEM_A + i * 16 + q, SEM_A + i * 16 + p, dev).start()
        return 0

    lax.fori_loop(0, 15, a_send, 0)

    def a_sent(k, _):
        for i in range(3):
            q = lax.rem(plane_index(i) + 1 + k, 16)
            sent(own_piece(i), SEM_A + i * 16 + q)
        return 0

    pending.append(lambda: lax.fori_loop(0, 15, a_sent, 0))

    wcols = (pl.ds(0, HALF), pl.ds(HALF, HALF))

    def w_one(k, d, part=None):
        rows = slice(None) if part is None else pl.ds(16 * part, 16)
        at = (zs[d], y) if k == 0 else (z, ys[d])
        return WM.at[at[0], at[1], rows, wcols[k]]

    def w_line(k, d, part=None):
        group = slice(None) if part is None else pl.ds(2 * part, 2)
        if k == 0:
            return WM.at[group, ys[d], :, wcols[k]]
        return WM.at[zs[d], group, :, wcols[k]]

    def w_send(view, axis, k, d, step, n):
        dev = (peer((d, 0, 0) if axis == 0 else (0, d, 0)), c)
        n = SEM_W + n * 2 + k
        send(view(k, *step), view(k, *step), n, n, dev).start()
        pending.append(lambda: sent(view(k, *step), n))

    def w_start(view, flip, n):
        for k in range(2):
            w_send(view, k ^ flip, k, 1, (0,), n)
            w_send(view, k ^ flip, k, 3, (0,), n + 1)

    def w_relay(view, flip, n):
        for k in range(2):
            got(view(k, 3), SEM_W + n * 2 + k)
            w_send(view, k ^ flip, k, 1, (3, 0), n + 2)
            got(view(k, 1), SEM_W + (n + 1) * 2 + k)
            w_send(view, k ^ flip, k, 3, (1, 1), n + 3)

    def w_end(view, n):
        for k in range(2):
            got(view(k, 2, 0), SEM_W + (n + 2) * 2 + k)
            got(view(k, 2, 1), SEM_W + (n + 3) * 2 + k)

    wcopy.wait()
    w_start(w_one, 0, 0)

    for n in ("wi", "wo", "wst", "sb", "dr", "eld", "it", "ot", "pi", "po"):
        loads[n].wait()
    in_rows = dot(normed, v["wi"][...]).astype(BF)
    out_rows = dot(normed, v["wo"][...]).astype(BF)
    step_raw = dot(normed, v["wst"][...], NT)

    def conv(prior, fresh, taps):
        t = taps[...]
        total = fresh * t[3:4]
        for j in range(3):
            total = total + prior[j].astype(F32) * t[j : j + 1]
        return silu(total)

    b_conv = conv(v["pi"], in_rows.astype(F32), v["it"])
    c_conv = conv(v["po"], out_rows.astype(F32), v["ot"])
    BV[...] = b_conv
    pre = step_raw + v["sb"][...]
    dt = jnp.maximum(pre, 0.0) + jnp.log(1.0 + jnp.exp(-jnp.abs(pre)))
    dec = jnp.exp(-dt * v["dr"][...] + v["eld"][...])
    c_hi, c_lo = split_bf(c_conv)
    CC[...] = jnp.concatenate([c_hi.astype(F32), c_lo.astype(F32)], axis=0).astype(BF)

    def plane(i, line, h=None):
        part = slice(None) if h is None else pl.ds(2 * h, 2)
        if i == 0:
            return X.at[c, line, part, :, :, cols(i)]
        if i == 1:
            return X.at[c, part, line, :, :, cols(i)]
        return X.at[c, part, :, line, :, cols(i)]

    def line_peer(i, d):
        there = list(own)
        there[i] = (own[i] + d) % 4
        return (ep_of(*there), c)

    def line_send(i, line, h, d, k):
        src = plane(i, line, h)
        k = SEM_B + i * 6 + k
        send(src, src, k, k, line_peer(i, d)).start()
        pending.append(lambda: sent(plane(i, line, h), k))

    def hand_over(i, d):
        line = (own[i] + d) % 4
        k = SEM_F + i * 4 + d
        send(plane(i, line), plane(i, line), k, k, (e, oc)).start()
        pending.append(lambda: sent(plane(i, line), k))

    def a_got(k, _):
        for i in range(3):
            q = lax.rem(plane_index(i) + 1 + k, 16)
            zz, yy, xx = coords(i, own[i], q)
            got(X.at[c, zz, yy, xx, :, cols(i)], SEM_A + i * 16 + q)
        return 0

    lax.fori_loop(0, 15, a_got, 0)
    for k, (h, d) in enumerate(((0, 1), (1, 3), (1, 1), (0, 3))):
        for i in range(3):
            line_send(i, own[i], h, d, k)
    for i in range(3):
        hand_over(i, 0)
    w_relay(w_one, 0, 0)

    loads["st"].wait()
    row = lax.broadcasted_iota(jnp.int32, (8, 512), 0)
    QR[...] = jnp.zeros((8, 2048), F32)

    def q_step(b, _):
        for g in range(4):
            s = v["st"][b, g * 512 : (g + 1) * 512, :].astype(BF)
            r = dot(CC[:, g * 128 : (g + 1) * 128], s, NT)
            sl = pl.ds(g * 512, 512)
            QR[:, sl] = jnp.where(row == b, r[0:8] + r[8:16], QR[:, sl])
        return 0

    lax.fori_loop(0, 8, q_step, 0)

    d1 = dec.astype(BF)
    d2 = (dec - d1.astype(F32)).astype(BF)
    seq = lax.broadcasted_iota(jnp.int32, (8, 1024), 1) // 128
    ones = (seq == lax.broadcasted_iota(jnp.int32, (8, 1024), 0)).astype(BF)
    spread_dec = dot(d1, ones, TN) + dot(d2, ones, TN)
    for b in range(8):
        DV[b] = spread_dec[:, b * 128 : (b + 1) * 128]

    loads["hs"].wait()
    spread = (
        lax.broadcasted_iota(jnp.int32, (32, 2048), 1) // 64
        == lax.broadcasted_iota(jnp.int32, (32, 2048), 0)
    ).astype(BF)
    heads = jnp.concatenate([dt, dec, jnp.broadcast_to(v["hs"][...], (8, 32))], axis=0)
    h1 = heads.astype(BF)
    r1 = heads - h1.astype(F32)
    h2 = r1.astype(BF)
    h3 = (r1 - h2.astype(F32)).astype(BF)
    wide = dot(h1, spread) + dot(h2, spread) + dot(h3, spread)
    dt_w, dec_w, skip_w = wide[0:8], wide[8:16], wide[16:24]
    bc = b_conv * c_conv
    bc_w = jnp.concatenate(
        [
            jnp.broadcast_to(
                jnp.sum(bc[:, g * 128 : (g + 1) * 128], axis=1, keepdims=True), (8, 512)
            )
            for g in range(4)
        ],
        axis=1,
    )
    kept = dec_w * QR[...]
    v_gain = dt_w * bc_w + skip_w

    for i in range(3):
        before, after = (own[i] + 3) % 4, (own[i] + 1) % 4
        got(plane(i, before, 0), SEM_B + i * 6)
        line_send(i, before, 0, 1, 4)
        got(plane(i, after, 1), SEM_B + i * 6 + 1)
        line_send(i, after, 1, 3, 5)
    for i in range(3):
        before, after = (own[i] + 3) % 4, (own[i] + 1) % 4
        got(plane(i, before, 1), SEM_B + i * 6 + 2)
        hand_over(i, 3)
        got(plane(i, after, 0), SEM_B + i * 6 + 3)
        hand_over(i, 1)
    for i in range(3):
        across = (own[i] + 2) % 4
        got(plane(i, across, 0), SEM_B + i * 6 + 4)
        got(plane(i, across, 1), SEM_B + i * 6 + 5)
        hand_over(i, 2)
    gcopy.wait()
    for w in vcopies:
        w.wait()
    proj = jnp.zeros((512, 128), F32)
    for i in range(3):
        for d in range(4):
            line = (own[i] + d) % 4
            view = X.at[oc]
            if i == 0:
                view = view.at[line, :, :, :, cols(i)]
            elif i == 1:
                view = view.at[:, line, :, :, cols(i)]
            else:
                view = view.at[:, :, line, :, cols(i)]
            got(view, SEM_F + i * 4 + d)
        at, width = PIECES[i]
        for h in range(2):
            w = WGV[:, :, h * HALF + at : h * HALF + at + width].reshape(128, width)
            proj = proj + dot(X[h, :, :, :, :, at : at + width].reshape(512, width), w, NT)
    SP[...] = proj.reshape(64, 8, 128).astype(BF)

    for d in FAR:
        q = peer(d)
        send(SP.at[q], R1.at[e], SEM_P + q, SEM_P + e, (q, c)).start()

    def p_sent(k, _):
        q = lax.rem(e + 1 + k, 64)
        sent(SP.at[q], SEM_P + q)
        return 0

    pending.append(lambda: lax.fori_loop(0, 63, p_sent, 0))
    w_end(w_one, 0)
    w_start(w_line, 1, 4)
    R1[e] = SP[e]

    loads["routes"].wait()
    loads["cw"].wait()
    lane8 = lax.broadcasted_iota(jnp.int32, (8, 128), 1)
    hit = jnp.zeros((8, 128), F32)
    wgt = jnp.zeros((8, 128), F32)
    rt = v["routes"][...]
    cwv = v["cw"][...]
    for k in range(6):
        eq = lane8 == rt[:, k : k + 1]
        hit = hit + jnp.where(eq, 1.0, 0.0)
        wgt = wgt + jnp.where(eq, cwv[:, k : k + 1], 0.0)
    before = (
        lax.broadcasted_iota(jnp.int32, (8, 8), 0) > lax.broadcasted_iota(jnp.int32, (8, 8), 1)
    ).astype(BF)
    slot = dot(before, hit.astype(BF))
    s0 = jnp.where(slot < 0.5, 1.0, 0.0)
    w1 = wgt.astype(BF).astype(F32)
    w2 = wgt - w1
    rows6 = jnp.concatenate(
        [hit * s0, hit * (1 - s0), w1 * s0, w1 * (1 - s0), w2 * s0, w2 * (1 - s0)], axis=0
    ).astype(BF)
    place = (
        lax.broadcasted_iota(jnp.int32, (128, 1024), 1) // 16
        == lax.broadcasted_iota(jnp.int32, (128, 1024), 0)
    ).astype(BF)
    six = dot(rows6, place)
    lane_r = lax.broadcasted_iota(jnp.int32, (8, 1024), 1)
    first = (lane_r // 8) % 2 == 0
    hsel = jnp.where(first, six[0:8], six[8:16])
    w1s = jnp.where(first, six[16:24], six[24:32])
    w2s = jnp.where(first, six[32:40], six[40:48])
    tile = lane_r % 8
    zero = jnp.zeros((8, 1024), F32)

    def diag(a):
        return jnp.concatenate([jnp.where(tile == j, a, zero) for j in range(8)], axis=0)

    DM[...] = jnp.concatenate([diag(hsel), jnp.zeros((64, 1024), F32)], axis=0).T.astype(BF)
    CM[...] = jnp.concatenate([diag(w1s), diag(w2s)], axis=0).astype(BF)
    for n in ("vt", "pv", "gg"):
        loads[n].wait()

    for d in FAR[::-1]:
        q = peer(d)
        got(R1.at[q], SEM_P + q)

    gates, values = [], []
    for t in range(16):
        r = [R1[4 * t + j].astype(F32) for j in range(4)]
        gates.append(lane_groups(r, lane8))
        values.append(pltpu.roll(lane_groups([r[3], r[0], r[1], r[2]], lane8), 96, 1))
    gate = jnp.concatenate(gates, axis=1)
    value = jnp.concatenate(values, axis=1)
    value_rows = value.astype(BF)
    v_conv = conv(v["pv"], value, v["vt"])
    mixed = (kept + v_conv * v_gain) * silu(gate)
    normed_groups = []
    for g in range(4):
        m = mixed[:, g * 512 : (g + 1) * 512]
        normed_groups.append(m * lax.rsqrt(jnp.mean(m * m, axis=1, keepdims=True) + EPSILON))
    mixer_rows = jnp.concatenate(normed_groups, axis=1) * v["gg"][...]
    M[x] = mixer_rows.astype(BF)

    for d in (2, 1, 3):
        send(M.at[x], M.at[x], SEM_M + xs[d], SEM_M + x, (peer((0, 0, d)), c)).start()
        pending.append(lambda d=d: sent(M.at[x], SEM_M + xs[d]))
    w_relay(w_line, 1, 4)
    for new, old, fresh in ((nv_o, "pv", value_rows), (ni_o, "pi", in_rows), (no_o, "po", out_rows)):
        new[0] = v[old][1]
        new[1] = v[old][2]
        new[2] = fresh

    u = v_conv * dt_w
    u1 = u.astype(BF).astype(F32)
    pad = jnp.zeros((104, 2048), F32)
    UT[...] = jnp.concatenate([u1, u1, u - u1, pad], axis=0).T.astype(BF)

    def st_step(b, _):
        bv = BV[...]
        b1 = bv.astype(BF).astype(F32)
        keep = lax.broadcasted_iota(jnp.int32, (8, 512), 0) == b
        zero = jnp.zeros((8, 512), F32)
        k1, k2 = jnp.where(keep, b1, zero), jnp.where(keep, bv - b1, zero)
        rhs = jnp.concatenate([k1, k2, k1, jnp.zeros((104, 512), F32)], axis=0).astype(BF)
        for g in range(4):
            outer = dot(UT[g * 512 : (g + 1) * 512, :], rhs[:, g * 128 : (g + 1) * 128])
            for h in range(8):
                sl = pl.ds(g * 512 + h * 64, 64)
                keep_h = DV[b, pl.ds(g * 8 + h, 1), :]
                st_o[b, sl, :] = keep_h * v["st"][b, sl, :] + outer[h * 64 : (h + 1) * 64]
        return 0

    lax.fori_loop(0, 8, st_step, 0)
    finish()
    for d in (1, 3, 2):
        got(M.at[xs[d]], SEM_M + xs[d])
    w_end(w_line, 4)
    part = dot(M[...].reshape(32, 2048), WM[...].reshape(512, 2048), NT)
    SQ[...] = part.reshape(4, 8, 512).astype(BF)
    mine = c * 4 + x
    for d in (2, 1, 3, 0):
        q = xs[d]
        for other in (oc, c):
            if d == 0 and other is c:
                continue
            k = SEM_Q + q * 2 + other
            send(SQ.at[q], R2.at[mine], k, SEM_Q + mine, (peer((0, 0, d)), other)).start()
            pending.append(lambda q=q, k=k: sent(SQ.at[q], k))
    R2[mine] = SQ[x]
    for d in (0, 1, 3, 2):
        for other in (oc, c):
            if d == 0 and other is c:
                continue
            k = other * 4 + xs[d]
            got(R2.at[k], SEM_Q + k)
    tiles = [None] * 16
    a = [
        (R2[xx].astype(F32) + R2[4 + xx].astype(F32)).astype(BF).astype(F32) for xx in range(4)
    ]
    for zz in range(4):
        for yy in range(4):
            moved = [
                b[:, zz * 128 : (zz + 1) * 128]
                if xx == yy
                else pltpu.roll(b[:, zz * 128 : (zz + 1) * 128], (32 * (xx - yy)) % 128, 1)
                for xx, b in enumerate(a)
            ]
            tiles[zz * 4 + yy] = lane_groups(moved, lane8)
    mixed_out = jnp.concatenate(tiles, axis=1)
    loads["g2"].wait()
    stream = (tok + mixed_out).astype(BF).astype(F32)
    ffn = rms(stream, v["g2"][...]).astype(BF)
    ff32 = ffn.astype(F32)

    half = jnp.where(c == 0, ff32[:, :HALF], ff32[:, HALF:])
    stacked = jnp.concatenate([half[:, j * 128 : (j + 1) * 128] for j in range(8)], axis=0)
    FF[...] = jnp.concatenate([stacked, jnp.zeros((64, 128), F32)], axis=0).astype(BF)
    SD[...] = dot(DM[...], FF[...]).reshape(64, 16, 128).astype(BF)

    for d in FAR:
        q = peer(d)
        send(SD.at[q], RX.at[c, e], SEM_X + q, SEM_X + e, (q, c)).start()

    def x_sent(k, _):
        q = lax.rem(e + 1 + k, 64)
        sent(SD.at[q], SEM_X + q)
        return 0

    pending.append(lambda: lax.fori_loop(0, 63, x_sent, 0))
    RX[c, e] = SD[e]

    for n in ("cg", "cu", "cd"):
        loads[n].wait()
    sh = (silu(dot(ffn, v["cg"][...])) * dot(ffn, v["cu"][...])).astype(BF)
    shared = dot(sh, v["cd"][...]).astype(BF)
    SHS[...] = shared
    send(SHS, SHR, SEM_SH, SEM_SH, (e, oc)).start()
    pending.append(lambda: sent(SHS, SEM_SH))
    for n in ("rg", "ru", "rd"):
        loads[n].wait()

    def x_plane(h, dz):
        return RX.at[h, pl.ds(pl.multiple_of(zs[dz] * 16, 16), 16)]

    for dz in (0, 1, 3, 2):
        for d in FAR[::-1]:
            if d[0] == dz:
                q = peer(d)
                got(RX.at[c, q], SEM_X + q)
        send(x_plane(c, dz), x_plane(c, dz), SEM_FX + dz, SEM_FX + dz, (e, oc)).start()
        pending.append(lambda dz=dz: sent(x_plane(c, dz), SEM_FX + dz))
    for dz in (0, 1, 3, 2):
        got(x_plane(oc, dz), SEM_FX + dz)
    lhs = []
    for h in range(2):
        XF[...] = RX[h].astype(F32).reshape(1024, 128)
        for j in range(8):
            lhs.append(XF[pl.ds(j, 128, stride=8), :].astype(BF))
    rows = jnp.concatenate(lhs, axis=1)
    hid = (silu(dot(rows, v["rg"][...])) * dot(rows, v["ru"][...])).astype(BF)
    theirs = pl.ds(pl.multiple_of(oc * HALF, HALF), HALF)
    ours = pl.ds(pl.multiple_of(c * HALF, HALF), HALF)
    YS[...] = dot(hid, v["rd"][:, theirs]).astype(BF)
    send(YS, YR, SEM_YE, SEM_YE, (e, oc)).start()
    pending.append(lambda: sent(YS, SEM_YE))
    part_y = dot(hid, v["rd"][:, ours]).astype(BF).astype(F32)
    got(YR, SEM_YE)
    total_y = part_y + YR[...].astype(F32)
    for j in range(8):
        XF[pl.ds(j, 128, stride=8), :] = total_y[:, j * 128 : (j + 1) * 128]
    SY[...] = XF[...].reshape(64, 16, 128).astype(BF)

    for d in FAR:
        q = peer(d)
        send(SY.at[q], RY.at[e], SEM_Y + q, SEM_Y + e, (q, c)).start()

    def y_sent(k, _):
        q = lax.rem(e + 1 + k, 64)
        sent(SY.at[q], SEM_Y + q)
        return 0

    pending.append(lambda: lax.fori_loop(0, 63, y_sent, 0))
    RY[e] = SY[e]
    got(SHR, SEM_SH)
    resid = stream + (shared.astype(F32) + SHR[...].astype(F32))
    resid_half = jnp.where(c == 0, resid[:, :HALF], resid[:, HALF:])

    while len(pending) > 1:
        pending.pop(0)()
    for d in FAR[::-1]:
        q = peer(d)
        got(RY.at[q], SEM_Y + q)
    both = dot(CM[...], RY[...].reshape(1024, 128))
    comb = both[0:64] + both[64:128]
    routed = jnp.concatenate([comb[j * 8 : (j + 1) * 8] for j in range(8)], axis=1)
    res = (resid_half + routed).astype(BF)
    RES[...] = res
    send(RES, RESR, SEM_RF, SEM_RF, (e, oc)).start()
    pending.append(lambda: sent(RES, SEM_RF))
    res_o[:, ours] = res
    got(RESR, SEM_RF)
    res_o[:, theirs] = RESR[...]
    finish()


def store_kernel(*refs):
    n = len(refs) // 2
    sem = refs[-1]
    copies = []
    for k in range(n):
        src, dst = refs[k], refs[n + k]
        if k == 1:
            copies += [(src.at[b], dst.at[b]) for b in range(8)]
        else:
            copies.append((src, dst))
    started = [pltpu.make_async_copy(a, b, sem.at[k]) for k, (a, b) in enumerate(copies)]
    for w in started:
        w.start()
    for w in started:
        w.wait()


def shards(
    tokens,
    mixer_norm_gain,
    gate_projection_weight,
    value_projection_weight,
    input_projection_weight,
    output_projection_weight,
    step_projection_weight,
    head_step_bias,
    head_decay_rate,
    extra_log_decay,
    value_taps,
    input_taps,
    output_taps,
    prior_values,
    prior_input_maps,
    prior_output_maps,
    head_skip_gain,
    group_norm_gain,
    mixer_output_weight,
    recurrent_state,
    expert_norm_gain,
    routes,
    chosen_expert_weight,
    routed_gate_weight,
    routed_up_weight,
    routed_down_weight,
    common_gate_weight,
    common_up_weight,
    common_down_weight,
):
    pv, pi, po = (
        jnp.transpose(a, (1, 0, 2)) for a in (prior_values, prior_input_maps, prior_output_maps)
    )
    state = recurrent_state.reshape(8, 2048, 128)
    vals = dict(
        tok=tokens,
        g1=mixer_norm_gain[None],
        wi=input_projection_weight,
        wo=output_projection_weight,
        wst=step_projection_weight.T,
        sb=head_step_bias[None],
        dr=head_decay_rate[None],
        eld=extra_log_decay,
        vt=value_taps,
        it=input_taps,
        ot=output_taps,
        pv=pv,
        pi=pi,
        po=po,
        hs=head_skip_gain[None],
        gg=group_norm_gain[None],
        g2=expert_norm_gain[None],
        routes=routes,
        cw=chosen_expert_weight,
        rg=routed_gate_weight[0],
        ru=routed_up_weight[0],
        rd=routed_down_weight[0],
        cg=common_gate_weight,
        cu=common_up_weight,
        cd=common_down_weight,
        st=state,
    )
    ins = [vals[n] for n in LOADED] + [
        jnp.transpose(gate_projection_weight, (1, 2, 0))[0],
        jnp.transpose(value_projection_weight, (1, 2, 0))[0],
        mixer_output_weight.T,
    ]
    vm = pltpu.VMEM
    scratch = [vm(vals[n].shape, vals[n].dtype) for n in LOADED] + [
        vm((2, 4, 4, 4, 8, HALF), BF),
        vm((4, 32, 2048), BF),
        vm((4, 4, 32, 2048), BF),
        vm((64, 8, 128), BF),
        vm((64, 8, 128), BF),
        vm((4, 8, 2048), BF),
        vm((4, 8, 512), BF),
        vm((8, 8, 512), BF),
        vm((64, 16, 128), BF),
        vm((2, 64, 16, 128), BF),
        vm((1024, 128), F32),
        vm((128, HALF), BF),
        vm((128, HALF), BF),
        vm((64, 16, 128), BF),
        vm((64, 16, 128), BF),
        vm((8, 2048), BF),
        vm((8, 2048), BF),
        vm((8, HALF), BF),
        vm((8, HALF), BF),
        vm((1024, 128), BF),
        vm((128, 1024), BF),
        vm((8, 2048), F32),
        vm((16, 512), BF),
        vm((128, 128), BF),
        vm((8, 512), F32),
        vm((8, 32, 128), F32),
        vm((2048, 128), BF),
        pltpu.SemaphoreType.DMA((len(LOADED) + 5,)),
        pltpu.SemaphoreType.DMA((SEM_COUNT,)),
        pltpu.SemaphoreType.DMA((SEM_COUNT,)),
    ]
    shapes = [
        ((8, 2048), BF),
        ((8, 2048, 128), F32),
        ((3, 8, 2048), BF),
        ((3, 8, 512), BF),
        ((3, 8, 512), BF),
    ]
    held = pl.pallas_call(
        layer_kernel,
        out_shape=[pltpu.VMEM(a, t) for a, t in shapes],
        in_specs=[pl.BlockSpec(memory_space=pltpu.HBM)] * len(ins),
        out_specs=[pl.BlockSpec(memory_space=pltpu.VMEM)] * 5,
        scratch_shapes=scratch,
        compiler_params=pltpu.CompilerParams(
            collective_id=0, has_side_effects=True, vmem_limit_bytes=50 * 2**20
        ),
    )(*ins)
    result, state_next, nv, ni, no = pl.pallas_call(
        store_kernel,
        out_shape=[jax.ShapeDtypeStruct(a, t) for a, t in shapes],
        in_specs=[pl.BlockSpec(memory_space=pl.ANY)] * 5,
        out_specs=[pl.BlockSpec(memory_space=pltpu.HBM)] * 5,
        scratch_shapes=[pltpu.SemaphoreType.DMA((12,))],
        compiler_params=pltpu.CompilerParams(vmem_limit_bytes=2**20),
    )(*held)
    return (
        result,
        state_next.reshape(8, 32, 64, 128),
        jnp.transpose(nv, (1, 0, 2)),
        jnp.transpose(ni, (1, 0, 2)),
        jnp.transpose(no, (1, 0, 2)),
    )


def solution(mesh):
    return jax.shard_map(
        shards,
        mesh=mesh,
        in_specs=(
            P("ep", None),
            P(),
            P(None, "tp", "ep"),
            P(None, "tp", "ep"),
            P(None, "tp"),
            P(None, "tp"),
            P(None, "tp"),
            P("tp"),
            P("tp"),
            P("ep", "tp"),
            P(None, "tp"),
            P(None, "tp"),
            P(None, "tp"),
            P("ep", None, "tp"),
            P("ep", None, "tp"),
            P("ep", None, "tp"),
            P("tp"),
            P("tp"),
            P("tp", "ep"),
            P("ep", "tp", None, None),
            P(),
            P("ep", None),
            P("ep", None),
            P("ep", None, "tp"),
            P("ep", None, "tp"),
            P("ep", "tp", None),
            P(None, "tp"),
            P(None, "tp"),
            P("tp", None),
        ),
        out_specs=(
            P("ep", None),
            P("ep", "tp", None, None),
            P("ep", None, "tp"),
            P("ep", None, "tp"),
            P("ep", None, "tp"),
        ),
        check_vma=False,
    )
```

```python
import functools

import jax
import jax.numpy as jnp
from jax import lax
from jax.experimental import pallas as pl
from jax.experimental.pallas import tpu as pltpu
from jax.sharding import PartitionSpec as P

MESH = pl.DeviceIdType.MESH
EPSILON = 1e-06
BF, F32 = jnp.bfloat16, jnp.float32
NT = (((1,), (1,)), ((), ()))
TN = (((0,), (0,)), ((), ()))
HALF = 1024
PIECES = ((0, 256), (256, 384), (640, 384))

SEM_A = 0
SEM_B = SEM_A + 48
SEM_F = SEM_B + 18
SEM_P = SEM_F + 12
SEM_W = SEM_P + 64
SEM_M = SEM_W + 16
SEM_Q = SEM_M + 4
SEM_X = SEM_Q + 8
SEM_Y = SEM_X + 64
SEM_FX = SEM_Y + 64
SEM_SH = SEM_FX + 4
SEM_YE = SEM_SH + 1
SEM_RF = SEM_YE + 1
SEM_COUNT = SEM_RF + 1

def hops(d):
    return sum(min(k, 4 - k) for k in d)


FAR = sorted(
    [(i // 16, i // 4 % 4, i % 4) for i in range(1, 64)], key=hops, reverse=True
)

LOADED = (
    "tok", "g1", "wi", "wo", "wst", "sb", "dr", "eld", "vt", "it", "ot", "pv", "pi", "po", "hs",
    "gg", "g2", "routes", "cw", "rg", "ru", "rd", "cg", "cu", "cd", "st",
)


def silu(x):
    return x * (1.0 / (1.0 + jnp.exp(-x)))


def rms(x, gain):
    return x * lax.rsqrt(jnp.mean(x * x, axis=-1, keepdims=True) + EPSILON) * gain


def split_bf(x):
    hi = x.astype(BF)
    return hi, (x - hi.astype(F32)).astype(BF)


def dot(a, b, dims=(((1,), (0,)), ((), ()))):
    return lax.dot_general(a, b, dims, preferred_element_type=F32)


def lane_groups(pieces, lane):
    return jnp.where(
        lane < 32,
        pieces[0],
        jnp.where(lane < 64, pieces[1], jnp.where(lane < 96, pieces[2], pieces[3])),
    )


def layer_kernel(*refs):
    hbm = dict(zip(LOADED + ("gt", "vtp", "wmt"), refs[:29]))
    res_o, st_o, nv_o, ni_o, no_o = refs[29:34]
    v = dict(zip(LOADED, refs[34:60]))
    (
        X, WGV, WM, SP, R1, M, SQ, R2, SD, RX, XF, YS, YR, SY, RY, SHS, SHR, RES, RESR, DM, CM, QR,
        CC, FF, BV, DV, UT, ld, ss, rs,
    ) = refs[60:]

    e = lax.axis_index("ep")
    c = lax.axis_index("tp")
    oc = 1 - c
    z, y, x = e // 16, (e // 4) % 4, e % 4
    own = (z, y, x)

    def ep_of(zz, yy, xx):
        return zz * 16 + yy * 4 + xx

    def send(src, dst, so, ro, dev):
        return pltpu.make_async_remote_copy(
            src_ref=src, dst_ref=dst, send_sem=ss.at[so], recv_sem=rs.at[ro],
            device_id=dev, device_id_type=MESH,
        )

    def got(dst, ro):
        send(dst, dst, ro, ro, (e, oc)).wait_recv()

    def sent(src, so):
        send(src, src, so, so, (e, oc)).wait_send()

    pending = []

    def finish():
        for f in pending:
            f()
        pending.clear()

    loads = {}
    for k, n in enumerate(LOADED):
        loads[n] = pltpu.make_async_copy(hbm[n], v[n], ld.at[k])
    base = len(LOADED)
    gcopy = pltpu.make_async_copy(hbm["gt"], WGV.at[x], ld.at[base])
    vcopies = [
        pltpu.make_async_copy(hbm["vtp"], WGV.at[(x + 1 + j) % 4], ld.at[base + 1 + j])
        for j in range(3)
    ]
    wcopy = pltpu.make_async_copy(hbm["wmt"], WM.at[z, y], ld.at[base + 4])
    loads["tok"].start()
    loads["g1"].start()
    bar = pltpu.get_barrier_semaphore()
    pl.semaphore_signal(bar, inc=1, device_id=(e, oc), device_id_type=MESH)

    zs, ys, xs = ([(w + d) % 4 for d in range(4)] for w in own)

    def peer(d):
        return zs[d[0]] * 16 + ys[d[1]] * 4 + xs[d[2]]

    greeted = [d for d in FAR if 0 in d]
    for d in greeted:
        pl.semaphore_signal(bar, inc=1, device_id=(peer(d), c), device_id_type=MESH)

    wcopy.start()
    loads["wst"].start()
    for n in ("wi", "wo", "sb", "dr", "eld", "vt", "it", "ot", "pv", "pi", "po", "hs", "gg", "g2", "routes", "cw"):
        loads[n].start()
    gcopy.start()
    for w in vcopies:
        w.start()
    for n in ("st", "cg", "cu", "cd", "rg", "ru", "rd"):
        loads[n].start()

    loads["tok"].wait()
    loads["g1"].wait()
    tok = v["tok"][...].astype(F32)
    normed = rms(tok, v["g1"][...]).astype(BF)
    nf = normed.astype(F32)
    X[c, z, y, x] = jnp.where(c == 0, nf[:, :HALF], nf[:, HALF:]).astype(BF)

    pl.semaphore_wait(bar, 1 + len(greeted))

    def coords(i, line, p):
        a, b = p // 4, p % 4
        return ((line, a, b), (a, line, b), (a, b, line))[i]

    def plane_index(i):
        return (y * 4 + x, z * 4 + x, z * 4 + y)[i]

    def cols(i):
        return pl.ds(PIECES[i][0], PIECES[i][1])

    def own_piece(i):
        return X.at[c, z, y, x, :, cols(i)]

    flat = sorted([(k // 4, k % 4) for k in range(1, 16)], key=hops, reverse=True)

    def piece_peer(i, d):
        full = [d[0], d[1]]
        full.insert(i, 0)
        return full, plane_index_of(i, full)

    def plane_index_of(i, f):
        a, b = [(zs, ys, xs)[k][f[k]] for k in range(3) if k != i]
        return a * 4 + b

    for d in flat:
        for i in range(3):
            full, q = piece_peer(i, d)
            send(own_piece(i), own_piece(i), SEM_A + i * 16 + q, SEM_A + i * 16 + plane_index(i), (peer(full), c)).start()

    def a_sent(k, _):
        for i in range(3):
            q = lax.rem(plane_index(i) + 1 + k, 16)
            sent(own_piece(i), SEM_A + i * 16 + q)
        return 0

    pending.append(lambda: lax.fori_loop(0, 15, a_sent, 0))

    wcols = (pl.ds(0, HALF), pl.ds(HALF, HALF))

    def w_one(k, d, part=None):
        rows = slice(None) if part is None else pl.ds(16 * part, 16)
        at = (zs[d], y) if k == 0 else (z, ys[d])
        return WM.at[at[0], at[1], rows, wcols[k]]

    def w_line(k, d, part=None):
        group = slice(None) if part is None else pl.ds(2 * part, 2)
        if k == 0:
            return WM.at[group, ys[d], :, wcols[k]]
        return WM.at[zs[d], group, :, wcols[k]]

    def w_send(view, axis, k, d, step, n):
        dev = (peer((d, 0, 0) if axis == 0 else (0, d, 0)), c)
        n = SEM_W + n * 2 + k
        send(view(k, *step), view(k, *step), n, n, dev).start()
        pending.append(lambda: sent(view(k, *step), n))

    def w_start(view, flip, n):
        for k in range(2):
            w_send(view, k ^ flip, k, 1, (0,), n)
            w_send(view, k ^ flip, k, 3, (0,), n + 1)

    def w_relay(view, flip, n):
        for k in range(2):
            got(view(k, 3), SEM_W + n * 2 + k)
            w_send(view, k ^ flip, k, 1, (3, 0), n + 2)
            got(view(k, 1), SEM_W + (n + 1) * 2 + k)
            w_send(view, k ^ flip, k, 3, (1, 1), n + 3)

    def w_end(view, n):
        for k in range(2):
            got(view(k, 2, 0), SEM_W + (n + 2) * 2 + k)
            got(view(k, 2, 1), SEM_W + (n + 3) * 2 + k)

    wcopy.wait()
    w_start(w_one, 0, 0)

    for n in ("wi", "wo", "wst", "sb", "dr", "eld", "it", "ot", "pi", "po"):
        loads[n].wait()
    in_rows = dot(normed, v["wi"][...]).astype(BF)
    out_rows = dot(normed, v["wo"][...]).astype(BF)
    step_raw = dot(normed, v["wst"][...], NT)

    def conv(prior, fresh, taps):
        t = taps[...]
        total = fresh * t[3:4]
        for j in range(3):
            total = total + prior[j].astype(F32) * t[j : j + 1]
        return silu(total)

    b_conv = conv(v["pi"], in_rows.astype(F32), v["it"])
    c_conv = conv(v["po"], out_rows.astype(F32), v["ot"])
    BV[...] = b_conv
    pre = step_raw + v["sb"][...]
    dt = jnp.maximum(pre, 0.0) + jnp.log(1.0 + jnp.exp(-jnp.abs(pre)))
    dec = jnp.exp(-dt * v["dr"][...] + v["eld"][...])
    c_hi, c_lo = split_bf(c_conv)
    CC[...] = jnp.concatenate([c_hi.astype(F32), c_lo.astype(F32)], axis=0).astype(BF)

    def plane(i, line, h=None):
        part = slice(None) if h is None else pl.ds(2 * h, 2)
        if i == 0:
            return X.at[c, line, part, :, :, cols(i)]
        if i == 1:
            return X.at[c, part, line, :, :, cols(i)]
        return X.at[c, part, :, line, :, cols(i)]

    def line_peer(i, d):
        there = list(own)
        there[i] = (own[i] + d) % 4
        return (ep_of(*there), c)

    def line_send(i, line, h, d, k):
        src = plane(i, line, h)
        k = SEM_B + i * 6 + k
        send(src, src, k, k, line_peer(i, d)).start()
        pending.append(lambda: sent(plane(i, line, h), k))

    def hand_over(i, d):
        line = (own[i] + d) % 4
        k = SEM_F + i * 4 + d
        send(plane(i, line), plane(i, line), k, k, (e, oc)).start()
        pending.append(lambda: sent(plane(i, line), k))

    for d in flat[::-1]:
        for i in range(3):
            full, q = piece_peer(i, d)
            got(X.at[c, zs[full[0]], ys[full[1]], xs[full[2]], :, cols(i)], SEM_A + i * 16 + q)
    for k, (h, d) in enumerate(((0, 1), (1, 3), (1, 1), (0, 3))):
        for i in range(3):
            line_send(i, own[i], h, d, k)
    for i in range(3):
        hand_over(i, 0)
    w_relay(w_one, 0, 0)

    loads["st"].wait()
    row = lax.broadcasted_iota(jnp.int32, (8, 512), 0)
    QR[...] = jnp.zeros((8, 2048), F32)

    def q_step(b, _):
        for g in range(4):
            s = v["st"][b, g * 512 : (g + 1) * 512, :].astype(BF)
            r = dot(CC[:, g * 128 : (g + 1) * 128], s, NT)
            sl = pl.ds(g * 512, 512)
            QR[:, sl] = jnp.where(row == b, r[0:8] + r[8:16], QR[:, sl])
        return 0

    lax.fori_loop(0, 8, q_step, 0)

    d1 = dec.astype(BF)
    d2 = (dec - d1.astype(F32)).astype(BF)
    seq = lax.broadcasted_iota(jnp.int32, (8, 1024), 1) // 128
    ones = (seq == lax.broadcasted_iota(jnp.int32, (8, 1024), 0)).astype(BF)
    spread_dec = dot(d1, ones, TN) + dot(d2, ones, TN)
    for b in range(8):
        DV[b] = spread_dec[:, b * 128 : (b + 1) * 128]

    loads["hs"].wait()
    spread = (
        lax.broadcasted_iota(jnp.int32, (32, 2048), 1) // 64
        == lax.broadcasted_iota(jnp.int32, (32, 2048), 0)
    ).astype(BF)
    heads = jnp.concatenate([dt, dec, jnp.broadcast_to(v["hs"][...], (8, 32))], axis=0)
    h1 = heads.astype(BF)
    r1 = heads - h1.astype(F32)
    h2 = r1.astype(BF)
    h3 = (r1 - h2.astype(F32)).astype(BF)
    wide = dot(h1, spread) + dot(h2, spread) + dot(h3, spread)
    dt_w, dec_w, skip_w = wide[0:8], wide[8:16], wide[16:24]
    bc = b_conv * c_conv
    bc_w = jnp.concatenate(
        [
            jnp.broadcast_to(
                jnp.sum(bc[:, g * 128 : (g + 1) * 128], axis=1, keepdims=True), (8, 512)
            )
            for g in range(4)
        ],
        axis=1,
    )
    kept = dec_w * QR[...]
    v_gain = dt_w * bc_w + skip_w

    for i in range(3):
        before, after = (own[i] + 3) % 4, (own[i] + 1) % 4
        got(plane(i, before, 0), SEM_B + i * 6)
        line_send(i, before, 0, 1, 4)
        got(plane(i, after, 1), SEM_B + i * 6 + 1)
        line_send(i, after, 1, 3, 5)
    for i in range(3):
        before, after = (own[i] + 3) % 4, (own[i] + 1) % 4
        got(plane(i, before, 1), SEM_B + i * 6 + 2)
        hand_over(i, 3)
        got(plane(i, after, 0), SEM_B + i * 6 + 3)
        hand_over(i, 1)
    for i in range(3):
        across = (own[i] + 2) % 4
        got(plane(i, across, 0), SEM_B + i * 6 + 4)
        got(plane(i, across, 1), SEM_B + i * 6 + 5)
        hand_over(i, 2)
    w_end(w_one, 0)
    w_start(w_line, 1, 4)
    gcopy.wait()
    for w in vcopies:
        w.wait()
    proj = jnp.zeros((512, 128), F32)
    for i in range(3):
        for d in range(4):
            line = (own[i] + d) % 4
            view = X.at[oc]
            if i == 0:
                view = view.at[line, :, :, :, cols(i)]
            elif i == 1:
                view = view.at[:, line, :, :, cols(i)]
            else:
                view = view.at[:, :, line, :, cols(i)]
            got(view, SEM_F + i * 4 + d)
        at, width = PIECES[i]
        for h in range(2):
            w = WGV[:, :, h * HALF + at : h * HALF + at + width].reshape(128, width)
            proj = proj + dot(X[h, :, :, :, :, at : at + width].reshape(512, width), w, NT)
    SP[...] = proj.reshape(64, 8, 128).astype(BF)

    for d in FAR:
        q = peer(d)
        send(SP.at[q], R1.at[e], SEM_P + q, SEM_P + e, (q, c)).start()

    def p_sent(k, _):
        q = lax.rem(e + 1 + k, 64)
        sent(SP.at[q], SEM_P + q)
        return 0

    pending.append(lambda: lax.fori_loop(0, 63, p_sent, 0))
    R1[e] = SP[e]

    loads["routes"].wait()
    loads["cw"].wait()
    lane8 = lax.broadcasted_iota(jnp.int32, (8, 128), 1)
    hit = jnp.zeros((8, 128), F32)
    wgt = jnp.zeros((8, 128), F32)
    rt = v["routes"][...]
    cwv = v["cw"][...]
    for k in range(6):
        eq = lane8 == rt[:, k : k + 1]
        hit = hit + jnp.where(eq, 1.0, 0.0)
        wgt = wgt + jnp.where(eq, cwv[:, k : k + 1], 0.0)
    before = (
        lax.broadcasted_iota(jnp.int32, (8, 8), 0) > lax.broadcasted_iota(jnp.int32, (8, 8), 1)
    ).astype(BF)
    slot = dot(before, hit.astype(BF))
    s0 = jnp.where(slot < 0.5, 1.0, 0.0)
    w1 = wgt.astype(BF).astype(F32)
    w2 = wgt - w1
    rows6 = jnp.concatenate(
        [hit * s0, hit * (1 - s0), w1 * s0, w1 * (1 - s0), w2 * s0, w2 * (1 - s0)], axis=0
    ).astype(BF)
    place = (
        lax.broadcasted_iota(jnp.int32, (128, 1024), 1) // 16
        == lax.broadcasted_iota(jnp.int32, (128, 1024), 0)
    ).astype(BF)
    six = dot(rows6, place)
    lane_r = lax.broadcasted_iota(jnp.int32, (8, 1024), 1)
    first = (lane_r // 8) % 2 == 0
    hsel = jnp.where(first, six[0:8], six[8:16])
    w1s = jnp.where(first, six[16:24], six[24:32])
    w2s = jnp.where(first, six[32:40], six[40:48])
    tile = lane_r % 8
    zero = jnp.zeros((8, 1024), F32)

    def diag(a):
        return jnp.concatenate([jnp.where(tile == j, a, zero) for j in range(8)], axis=0)

    DM[...] = jnp.concatenate([diag(hsel), jnp.zeros((64, 1024), F32)], axis=0).T.astype(BF)
    CM[...] = jnp.concatenate([diag(w1s), diag(w2s)], axis=0).astype(BF)
    for n in ("vt", "pv", "gg"):
        loads[n].wait()

    for d in FAR[::-1]:
        q = peer(d)
        got(R1.at[q], SEM_P + q)

    gates, values = [], []
    for t in range(16):
        r = [R1[4 * t + j].astype(F32) for j in range(4)]
        gates.append(lane_groups(r, lane8))
        values.append(pltpu.roll(lane_groups([r[3], r[0], r[1], r[2]], lane8), 96, 1))
    gate = jnp.concatenate(gates, axis=1)
    value = jnp.concatenate(values, axis=1)
    value_rows = value.astype(BF)
    v_conv = conv(v["pv"], value, v["vt"])
    mixed = (kept + v_conv * v_gain) * silu(gate)
    normed_groups = []
    for g in range(4):
        m = mixed[:, g * 512 : (g + 1) * 512]
        normed_groups.append(m * lax.rsqrt(jnp.mean(m * m, axis=1, keepdims=True) + EPSILON))
    mixer_rows = jnp.concatenate(normed_groups, axis=1) * v["gg"][...]
    M[x] = mixer_rows.astype(BF)

    for d in (2, 1, 3):
        send(M.at[x], M.at[x], SEM_M + xs[d], SEM_M + x, (peer((0, 0, d)), c)).start()
        pending.append(lambda d=d: sent(M.at[x], SEM_M + xs[d]))
    w_relay(w_line, 1, 4)
    for new, old, fresh in ((nv_o, "pv", value_rows), (ni_o, "pi", in_rows), (no_o, "po", out_rows)):
        new[0] = v[old][1]
        new[1] = v[old][2]
        new[2] = fresh

    u = v_conv * dt_w
    u1 = u.astype(BF).astype(F32)
    pad = jnp.zeros((104, 2048), F32)
    UT[...] = jnp.concatenate([u1, u1, u - u1, pad], axis=0).T.astype(BF)

    def st_step(b, _):
        bv = BV[...]
        b1 = bv.astype(BF).astype(F32)
        keep = lax.broadcasted_iota(jnp.int32, (8, 512), 0) == b
        zero = jnp.zeros((8, 512), F32)
        k1, k2 = jnp.where(keep, b1, zero), jnp.where(keep, bv - b1, zero)
        rhs = jnp.concatenate([k1, k2, k1, jnp.zeros((104, 512), F32)], axis=0).astype(BF)
        for g in range(4):
            outer = dot(UT[g * 512 : (g + 1) * 512, :], rhs[:, g * 128 : (g + 1) * 128])
            for h in range(8):
                sl = pl.ds(g * 512 + h * 64, 64)
                keep_h = DV[b, pl.ds(g * 8 + h, 1), :]
                st_o[b, sl, :] = keep_h * v["st"][b, sl, :] + outer[h * 64 : (h + 1) * 64]
        return 0

    lax.fori_loop(0, 8, st_step, 0)
    finish()
    for d in (1, 3, 2):
        got(M.at[xs[d]], SEM_M + xs[d])
    w_end(w_line, 4)
    part = dot(M[...].reshape(32, 2048), WM[...].reshape(512, 2048), NT)
    SQ[...] = part.reshape(4, 8, 512).astype(BF)
    mine = c * 4 + x
    for d in (2, 1, 3, 0):
        q = xs[d]
        for other in (oc, c):
            if d == 0 and other is c:
                continue
            k = SEM_Q + q * 2 + other
            send(SQ.at[q], R2.at[mine], k, SEM_Q + mine, (peer((0, 0, d)), other)).start()
            pending.append(lambda q=q, k=k: sent(SQ.at[q], k))
    R2[mine] = SQ[x]
    for d in (0, 1, 3, 2):
        for other in (oc, c):
            if d == 0 and other is c:
                continue
            k = other * 4 + xs[d]
            got(R2.at[k], SEM_Q + k)
    tiles = [None] * 16
    a = [
        (R2[xx].astype(F32) + R2[4 + xx].astype(F32)).astype(BF).astype(F32) for xx in range(4)
    ]
    for zz in range(4):
        for yy in range(4):
            moved = [
                b[:, zz * 128 : (zz + 1) * 128]
                if xx == yy
                else pltpu.roll(b[:, zz * 128 : (zz + 1) * 128], (32 * (xx - yy)) % 128, 1)
                for xx, b in enumerate(a)
            ]
            tiles[zz * 4 + yy] = lane_groups(moved, lane8)
    mixed_out = jnp.concatenate(tiles, axis=1)
    loads["g2"].wait()
    stream = (tok + mixed_out).astype(BF).astype(F32)
    ffn = rms(stream, v["g2"][...]).astype(BF)
    ff32 = ffn.astype(F32)

    half = jnp.where(c == 0, ff32[:, :HALF], ff32[:, HALF:])
    stacked = jnp.concatenate([half[:, j * 128 : (j + 1) * 128] for j in range(8)], axis=0)
    FF[...] = jnp.concatenate([stacked, jnp.zeros((64, 128), F32)], axis=0).astype(BF)
    SD[...] = dot(DM[...], FF[...]).reshape(64, 16, 128).astype(BF)

    for d in FAR:
        q = peer(d)
        send(SD.at[q], RX.at[c, e], SEM_X + q, SEM_X + e, (q, c)).start()

    def x_sent(k, _):
        q = lax.rem(e + 1 + k, 64)
        sent(SD.at[q], SEM_X + q)
        return 0

    pending.append(lambda: lax.fori_loop(0, 63, x_sent, 0))
    RX[c, e] = SD[e]

    for n in ("cg", "cu", "cd"):
        loads[n].wait()
    sh = (silu(dot(ffn, v["cg"][...])) * dot(ffn, v["cu"][...])).astype(BF)
    shared = dot(sh, v["cd"][...]).astype(BF)
    SHS[...] = shared
    send(SHS, SHR, SEM_SH, SEM_SH, (e, oc)).start()
    pending.append(lambda: sent(SHS, SEM_SH))
    for n in ("rg", "ru", "rd"):
        loads[n].wait()

    def x_plane(h, dz):
        return RX.at[h, pl.ds(pl.multiple_of(zs[dz] * 16, 16), 16)]

    for dz in (0, 1, 3, 2):
        for d in FAR[::-1]:
            if d[0] == dz:
                q = peer(d)
                got(RX.at[c, q], SEM_X + q)
        send(x_plane(c, dz), x_plane(c, dz), SEM_FX + dz, SEM_FX + dz, (e, oc)).start()
        pending.append(lambda dz=dz: sent(x_plane(c, dz), SEM_FX + dz))
    for dz in (0, 1, 3, 2):
        got(x_plane(oc, dz), SEM_FX + dz)
    lhs = []
    for h in range(2):
        XF[...] = RX[h].astype(F32).reshape(1024, 128)
        for j in range(8):
            lhs.append(XF[pl.ds(j, 128, stride=8), :].astype(BF))
    rows = jnp.concatenate(lhs, axis=1)
    hid = (silu(dot(rows, v["rg"][...])) * dot(rows, v["ru"][...])).astype(BF)
    theirs = pl.ds(pl.multiple_of(oc * HALF, HALF), HALF)
    ours = pl.ds(pl.multiple_of(c * HALF, HALF), HALF)
    YS[...] = dot(hid, v["rd"][:, theirs]).astype(BF)
    send(YS, YR, SEM_YE, SEM_YE, (e, oc)).start()
    pending.append(lambda: sent(YS, SEM_YE))
    part_y = dot(hid, v["rd"][:, ours]).astype(BF).astype(F32)
    got(YR, SEM_YE)
    total_y = part_y + YR[...].astype(F32)
    for j in range(8):
        XF[pl.ds(j, 128, stride=8), :] = total_y[:, j * 128 : (j + 1) * 128]
    SY[...] = XF[...].reshape(64, 16, 128).astype(BF)

    for d in FAR:
        q = peer(d)
        send(SY.at[q], RY.at[e], SEM_Y + q, SEM_Y + e, (q, c)).start()

    def y_sent(k, _):
        q = lax.rem(e + 1 + k, 64)
        sent(SY.at[q], SEM_Y + q)
        return 0

    pending.append(lambda: lax.fori_loop(0, 63, y_sent, 0))
    RY[e] = SY[e]
    got(SHR, SEM_SH)
    resid = stream + (shared.astype(F32) + SHR[...].astype(F32))
    resid_half = jnp.where(c == 0, resid[:, :HALF], resid[:, HALF:])

    while len(pending) > 1:
        pending.pop(0)()
    for d in FAR[::-1]:
        q = peer(d)
        got(RY.at[q], SEM_Y + q)
    both = dot(CM[...], RY[...].reshape(1024, 128))
    comb = both[0:64] + both[64:128]
    routed = jnp.concatenate([comb[j * 8 : (j + 1) * 8] for j in range(8)], axis=1)
    res = (resid_half + routed).astype(BF)
    RES[...] = res
    send(RES, RESR, SEM_RF, SEM_RF, (e, oc)).start()
    pending.append(lambda: sent(RES, SEM_RF))
    res_o[:, ours] = res
    got(RESR, SEM_RF)
    res_o[:, theirs] = RESR[...]
    finish()


def store_kernel(*refs):
    n = len(refs) // 2
    sem = refs[-1]
    copies = []
    for k in range(n):
        src, dst = refs[k], refs[n + k]
        if k == 1:
            copies += [(src.at[b], dst.at[b]) for b in range(8)]
        else:
            copies.append((src, dst))
    started = [pltpu.make_async_copy(a, b, sem.at[k]) for k, (a, b) in enumerate(copies)]
    for w in started:
        w.start()
    for w in started:
        w.wait()


def shards(
    tokens,
    mixer_norm_gain,
    gate_projection_weight,
    value_projection_weight,
    input_projection_weight,
    output_projection_weight,
    step_projection_weight,
    head_step_bias,
    head_decay_rate,
    extra_log_decay,
    value_taps,
    input_taps,
    output_taps,
    prior_values,
    prior_input_maps,
    prior_output_maps,
    head_skip_gain,
    group_norm_gain,
    mixer_output_weight,
    recurrent_state,
    expert_norm_gain,
    routes,
    chosen_expert_weight,
    routed_gate_weight,
    routed_up_weight,
    routed_down_weight,
    common_gate_weight,
    common_up_weight,
    common_down_weight,
):
    pv, pi, po = (
        jnp.transpose(a, (1, 0, 2)) for a in (prior_values, prior_input_maps, prior_output_maps)
    )
    state = recurrent_state.reshape(8, 2048, 128)
    vals = dict(
        tok=tokens,
        g1=mixer_norm_gain[None],
        wi=input_projection_weight,
        wo=output_projection_weight,
        wst=step_projection_weight.T,
        sb=head_step_bias[None],
        dr=head_decay_rate[None],
        eld=extra_log_decay,
        vt=value_taps,
        it=input_taps,
        ot=output_taps,
        pv=pv,
        pi=pi,
        po=po,
        hs=head_skip_gain[None],
        gg=group_norm_gain[None],
        g2=expert_norm_gain[None],
        routes=routes,
        cw=chosen_expert_weight,
        rg=routed_gate_weight[0],
        ru=routed_up_weight[0],
        rd=routed_down_weight[0],
        cg=common_gate_weight,
        cu=common_up_weight,
        cd=common_down_weight,
        st=state,
    )
    ins = [vals[n] for n in LOADED] + [
        jnp.transpose(gate_projection_weight, (1, 2, 0))[0],
        jnp.transpose(value_projection_weight, (1, 2, 0))[0],
        mixer_output_weight.T,
    ]
    vm = pltpu.VMEM
    scratch = [vm(vals[n].shape, vals[n].dtype) for n in LOADED] + [
        vm((2, 4, 4, 4, 8, HALF), BF),
        vm((4, 32, 2048), BF),
        vm((4, 4, 32, 2048), BF),
        vm((64, 8, 128), BF),
        vm((64, 8, 128), BF),
        vm((4, 8, 2048), BF),
        vm((4, 8, 512), BF),
        vm((8, 8, 512), BF),
        vm((64, 16, 128), BF),
        vm((2, 64, 16, 128), BF),
        vm((1024, 128), F32),
        vm((128, HALF), BF),
        vm((128, HALF), BF),
        vm((64, 16, 128), BF),
        vm((64, 16, 128), BF),
        vm((8, 2048), BF),
        vm((8, 2048), BF),
        vm((8, HALF), BF),
        vm((8, HALF), BF),
        vm((1024, 128), BF),
        vm((128, 1024), BF),
        vm((8, 2048), F32),
        vm((16, 512), BF),
        vm((128, 128), BF),
        vm((8, 512), F32),
        vm((8, 32, 128), F32),
        vm((2048, 128), BF),
        pltpu.SemaphoreType.DMA((len(LOADED) + 5,)),
        pltpu.SemaphoreType.DMA((SEM_COUNT,)),
        pltpu.SemaphoreType.DMA((SEM_COUNT,)),
    ]
    shapes = [
        ((8, 2048), BF),
        ((8, 2048, 128), F32),
        ((3, 8, 2048), BF),
        ((3, 8, 512), BF),
        ((3, 8, 512), BF),
    ]
    held = pl.pallas_call(
        layer_kernel,
        out_shape=[pltpu.VMEM(a, t) for a, t in shapes],
        in_specs=[pl.BlockSpec(memory_space=pltpu.HBM)] * len(ins),
        out_specs=[pl.BlockSpec(memory_space=pltpu.VMEM)] * 5,
        scratch_shapes=scratch,
        compiler_params=pltpu.CompilerParams(
            collective_id=0, has_side_effects=True, vmem_limit_bytes=50 * 2**20
        ),
    )(*ins)
    result, state_next, nv, ni, no = pl.pallas_call(
        store_kernel,
        out_shape=[jax.ShapeDtypeStruct(a, t) for a, t in shapes],
        in_specs=[pl.BlockSpec(memory_space=pl.ANY)] * 5,
        out_specs=[pl.BlockSpec(memory_space=pltpu.HBM)] * 5,
        scratch_shapes=[pltpu.SemaphoreType.DMA((12,))],
        compiler_params=pltpu.CompilerParams(vmem_limit_bytes=2**20),
    )(*held)
    return (
        result,
        state_next.reshape(8, 32, 64, 128),
        jnp.transpose(nv, (1, 0, 2)),
        jnp.transpose(ni, (1, 0, 2)),
        jnp.transpose(no, (1, 0, 2)),
    )


def solution(mesh):
    return jax.shard_map(
        shards,
        mesh=mesh,
        in_specs=(
            P("ep", None),
            P(),
            P(None, "tp", "ep"),
            P(None, "tp", "ep"),
            P(None, "tp"),
            P(None, "tp"),
            P(None, "tp"),
            P("tp"),
            P("tp"),
            P("ep", "tp"),
            P(None, "tp"),
            P(None, "tp"),
            P(None, "tp"),
            P("ep", None, "tp"),
            P("ep", None, "tp"),
            P("ep", None, "tp"),
            P("tp"),
            P("tp"),
            P("tp", "ep"),
            P("ep", "tp", None, None),
            P(),
            P("ep", None),
            P("ep", None),
            P("ep", None, "tp"),
            P("ep", None, "tp"),
            P("ep", "tp", None),
            P(None, "tp"),
            P(None, "tp"),
            P("tp", None),
        ),
        out_specs=(
            P("ep", None),
            P("ep", "tp", None, None),
            P("ep", None, "tp"),
            P("ep", None, "tp"),
            P("ep", None, "tp"),
        ),
        check_vma=False,
    )
```

```python
import functools

import jax
import jax.numpy as jnp
from jax import lax
from jax.experimental import pallas as pl
from jax.experimental.pallas import tpu as pltpu
from jax.sharding import PartitionSpec as P

MESH = pl.DeviceIdType.MESH
EPSILON = 1e-06
BF, F32 = jnp.bfloat16, jnp.float32
NT = (((1,), (1,)), ((), ()))
TN = (((0,), (0,)), ((), ()))
HALF = 1024
PIECES = ((0, 256), (256, 384), (640, 384))

SEM_A = 0
SEM_B = SEM_A + 48
SEM_F = SEM_B + 18
SEM_P = SEM_F + 12
SEM_W = SEM_P + 64
SEM_M = SEM_W + 16
SEM_Q = SEM_M + 4
SEM_X = SEM_Q + 8
SEM_Y = SEM_X + 64
SEM_FX = SEM_Y + 64
SEM_SH = SEM_FX + 4
SEM_YE = SEM_SH + 1
SEM_RF = SEM_YE + 1
SEM_COUNT = SEM_RF + 1

def hops(d):
    return sum(min(k, 4 - k) for k in d)


FAR = sorted(
    [(i // 16, i // 4 % 4, i % 4) for i in range(1, 64)], key=hops, reverse=True
)

LOADED = (
    "tok", "g1", "wi", "wo", "wst", "sb", "dr", "eld", "vt", "it", "ot", "pv", "pi", "po", "hs",
    "gg", "g2", "routes", "cw", "rg", "ru", "rd", "cg", "cu", "cd", "st",
)


def silu(x):
    return x * (1.0 / (1.0 + jnp.exp(-x)))


def rms(x, gain):
    return x * lax.rsqrt(jnp.mean(x * x, axis=-1, keepdims=True) + EPSILON) * gain


def split_bf(x):
    hi = x.astype(BF)
    return hi, (x - hi.astype(F32)).astype(BF)


def dot(a, b, dims=(((1,), (0,)), ((), ()))):
    return lax.dot_general(a, b, dims, preferred_element_type=F32)


def lane_groups(pieces, lane):
    return jnp.where(
        lane < 32,
        pieces[0],
        jnp.where(lane < 64, pieces[1], jnp.where(lane < 96, pieces[2], pieces[3])),
    )


def layer_kernel(*refs):
    hbm = dict(zip(LOADED + ("gt", "vtp", "wmt"), refs[:29]))
    res_o, st_o, nv_o, ni_o, no_o = refs[29:34]
    v = dict(zip(LOADED, refs[34:60]))
    (
        X, WGV, WM, SP, R1, M, SQ, R2, SD, RX, XF, YS, YR, SY, RY, SHS, SHR, RES, RESR, DM, CM, QR,
        CC, FF, BV, DV, UT, ld, ss, rs,
    ) = refs[60:]

    e = lax.axis_index("ep")
    c = lax.axis_index("tp")
    oc = 1 - c
    z, y, x = e // 16, (e // 4) % 4, e % 4
    own = (z, y, x)

    def ep_of(zz, yy, xx):
        return zz * 16 + yy * 4 + xx

    def send(src, dst, so, ro, dev):
        return pltpu.make_async_remote_copy(
            src_ref=src, dst_ref=dst, send_sem=ss.at[so], recv_sem=rs.at[ro],
            device_id=dev, device_id_type=MESH,
        )

    def got(dst, ro):
        send(dst, dst, ro, ro, (e, oc)).wait_recv()

    def sent(src, so):
        send(src, src, so, so, (e, oc)).wait_send()

    pending = []

    def finish():
        for f in pending:
            f()
        pending.clear()

    loads = {}
    for k, n in enumerate(LOADED):
        loads[n] = pltpu.make_async_copy(hbm[n], v[n], ld.at[k])
    base = len(LOADED)
    gcopy = pltpu.make_async_copy(hbm["gt"], WGV.at[x], ld.at[base])
    vcopies = [
        pltpu.make_async_copy(hbm["vtp"], WGV.at[(x + 1 + j) % 4], ld.at[base + 1 + j])
        for j in range(3)
    ]
    wcopy = pltpu.make_async_copy(hbm["wmt"], WM.at[z, y], ld.at[base + 4])
    loads["tok"].start()
    loads["g1"].start()
    bar = pltpu.get_barrier_semaphore()
    pl.semaphore_signal(bar, inc=1, device_id=(e, oc), device_id_type=MESH)

    zs, ys, xs = ([(w + d) % 4 for d in range(4)] for w in own)

    def peer(d):
        return zs[d[0]] * 16 + ys[d[1]] * 4 + xs[d[2]]

    greeted = [d for d in FAR if 0 in d]
    for d in greeted:
        pl.semaphore_signal(bar, inc=1, device_id=(peer(d), c), device_id_type=MESH)

    wcopy.start()
    loads["wst"].start()
    for n in ("wi", "wo", "sb", "dr", "eld", "vt", "it", "ot", "pv", "pi", "po", "hs", "gg", "g2", "routes", "cw"):
        loads[n].start()
    gcopy.start()
    for w in vcopies:
        w.start()
    for n in ("st", "cg", "cu", "cd", "rg", "ru", "rd"):
        loads[n].start()

    loads["tok"].wait()
    loads["g1"].wait()
    tok = v["tok"][...].astype(F32)
    normed = rms(tok, v["g1"][...]).astype(BF)
    nf = normed.astype(F32)
    X[c, z, y, x] = jnp.where(c == 0, nf[:, :HALF], nf[:, HALF:]).astype(BF)

    pl.semaphore_wait(bar, 1 + len(greeted))

    def coords(i, line, p):
        a, b = p // 4, p % 4
        return ((line, a, b), (a, line, b), (a, b, line))[i]

    def plane_index(i):
        return (y * 4 + x, z * 4 + x, z * 4 + y)[i]

    def cols(i):
        return pl.ds(PIECES[i][0], PIECES[i][1])

    def own_piece(i):
        return X.at[c, z, y, x, :, cols(i)]

    flat = sorted([(k // 4, k % 4) for k in range(1, 16)], key=hops, reverse=True)

    def piece_peer(i, d):
        full = [d[0], d[1]]
        full.insert(i, 0)
        return full, plane_index_of(i, full)

    def plane_index_of(i, f):
        a, b = [(zs, ys, xs)[k][f[k]] for k in range(3) if k != i]
        return a * 4 + b

    for d in flat:
        for i in range(3):
            full, q = piece_peer(i, d)
            send(own_piece(i), own_piece(i), SEM_A + i * 16 + q, SEM_A + i * 16 + plane_index(i), (peer(full), c)).start()

    def a_sent(k, _):
        for i in range(3):
            q = lax.rem(plane_index(i) + 1 + k, 16)
            sent(own_piece(i), SEM_A + i * 16 + q)
        return 0

    pending.append(lambda: lax.fori_loop(0, 15, a_sent, 0))

    wcols = (pl.ds(0, HALF), pl.ds(HALF, HALF))

    def w_one(k, d, part=None):
        rows = slice(None) if part is None else pl.ds(16 * part, 16)
        at = (zs[d], y) if k == 0 else (z, ys[d])
        return WM.at[at[0], at[1], rows, wcols[k]]

    def w_line(k, d, part=None):
        group = slice(None) if part is None else pl.ds(2 * part, 2)
        if k == 0:
            return WM.at[group, ys[d], :, wcols[k]]
        return WM.at[zs[d], group, :, wcols[k]]

    def w_send(view, axis, k, d, step, n):
        dev = (peer((d, 0, 0) if axis == 0 else (0, d, 0)), c)
        n = SEM_W + n * 2 + k
        send(view(k, *step), view(k, *step), n, n, dev).start()
        pending.append(lambda: sent(view(k, *step), n))

    def w_start(view, flip, n):
        for k in range(2):
            w_send(view, k ^ flip, k, 1, (0,), n)
            w_send(view, k ^ flip, k, 3, (0,), n + 1)

    def w_relay(view, flip, n):
        for k in range(2):
            got(view(k, 3), SEM_W + n * 2 + k)
            w_send(view, k ^ flip, k, 1, (3, 0), n + 2)
            got(view(k, 1), SEM_W + (n + 1) * 2 + k)
            w_send(view, k ^ flip, k, 3, (1, 1), n + 3)

    def w_end(view, n):
        for k in range(2):
            got(view(k, 2, 0), SEM_W + (n + 2) * 2 + k)
            got(view(k, 2, 1), SEM_W + (n + 3) * 2 + k)

    wcopy.wait()
    w_start(w_one, 0, 0)

    for n in ("wi", "wo", "wst", "sb", "dr", "eld", "it", "ot", "pi", "po"):
        loads[n].wait()
    in_rows = dot(normed, v["wi"][...]).astype(BF)
    out_rows = dot(normed, v["wo"][...]).astype(BF)
    step_raw = dot(normed, v["wst"][...], NT)

    def conv(prior, fresh, taps):
        t = taps[...]
        total = fresh * t[3:4]
        for j in range(3):
            total = total + prior[j].astype(F32) * t[j : j + 1]
        return silu(total)

    b_conv = conv(v["pi"], in_rows.astype(F32), v["it"])
    c_conv = conv(v["po"], out_rows.astype(F32), v["ot"])
    BV[...] = b_conv
    pre = step_raw + v["sb"][...]
    dt = jnp.maximum(pre, 0.0) + jnp.log(1.0 + jnp.exp(-jnp.abs(pre)))
    dec = jnp.exp(-dt * v["dr"][...] + v["eld"][...])
    c_hi, c_lo = split_bf(c_conv)
    CC[...] = jnp.concatenate([c_hi.astype(F32), c_lo.astype(F32)], axis=0).astype(BF)

    def plane(i, line, h=None):
        part = slice(None) if h is None else pl.ds(2 * h, 2)
        if i == 0:
            return X.at[c, line, part, :, :, cols(i)]
        if i == 1:
            return X.at[c, part, line, :, :, cols(i)]
        return X.at[c, part, :, line, :, cols(i)]

    def line_peer(i, d):
        there = list(own)
        there[i] = (own[i] + d) % 4
        return (ep_of(*there), c)

    def line_send(i, line, h, d, k):
        src = plane(i, line, h)
        k = SEM_B + i * 6 + k
        send(src, src, k, k, line_peer(i, d)).start()
        pending.append(lambda: sent(plane(i, line, h), k))

    def hand_over(i, d):
        line = (own[i] + d) % 4
        k = SEM_F + i * 4 + d
        send(plane(i, line), plane(i, line), k, k, (e, oc)).start()
        pending.append(lambda: sent(plane(i, line), k))

    for d in flat[::-1]:
        for i in range(3):
            full, q = piece_peer(i, d)
            got(X.at[c, zs[full[0]], ys[full[1]], xs[full[2]], :, cols(i)], SEM_A + i * 16 + q)
    for k, (h, d) in enumerate(((0, 1), (1, 3), (1, 1), (0, 3))):
        for i in range(3):
            line_send(i, own[i], h, d, k)
    for i in range(3):
        hand_over(i, 0)
    w_relay(w_one, 0, 0)

    loads["st"].wait()
    row = lax.broadcasted_iota(jnp.int32, (8, 512), 0)
    QR[...] = jnp.zeros((8, 2048), F32)

    def q_step(b, _):
        for g in range(4):
            s = v["st"][b, g * 512 : (g + 1) * 512, :].astype(BF)
            r = dot(CC[:, g * 128 : (g + 1) * 128], s, NT)
            sl = pl.ds(g * 512, 512)
            QR[:, sl] = jnp.where(row == b, r[0:8] + r[8:16], QR[:, sl])
        return 0

    lax.fori_loop(0, 8, q_step, 0)

    d1 = dec.astype(BF)
    d2 = (dec - d1.astype(F32)).astype(BF)
    seq = lax.broadcasted_iota(jnp.int32, (8, 1024), 1) // 128
    ones = (seq == lax.broadcasted_iota(jnp.int32, (8, 1024), 0)).astype(BF)
    spread_dec = dot(d1, ones, TN) + dot(d2, ones, TN)
    for b in range(8):
        DV[b] = spread_dec[:, b * 128 : (b + 1) * 128]

    loads["hs"].wait()
    spread = (
        lax.broadcasted_iota(jnp.int32, (32, 2048), 1) // 64
        == lax.broadcasted_iota(jnp.int32, (32, 2048), 0)
    ).astype(BF)
    heads = jnp.concatenate([dt, dec, jnp.broadcast_to(v["hs"][...], (8, 32))], axis=0)
    h1 = heads.astype(BF)
    r1 = heads - h1.astype(F32)
    h2 = r1.astype(BF)
    h3 = (r1 - h2.astype(F32)).astype(BF)
    wide = dot(h1, spread) + dot(h2, spread) + dot(h3, spread)
    dt_w, dec_w, skip_w = wide[0:8], wide[8:16], wide[16:24]
    bc = b_conv * c_conv
    bc_w = jnp.concatenate(
        [
            jnp.broadcast_to(
                jnp.sum(bc[:, g * 128 : (g + 1) * 128], axis=1, keepdims=True), (8, 512)
            )
            for g in range(4)
        ],
        axis=1,
    )
    kept = dec_w * QR[...]
    v_gain = dt_w * bc_w + skip_w

    for i in range(3):
        before, after = (own[i] + 3) % 4, (own[i] + 1) % 4
        got(plane(i, before, 0), SEM_B + i * 6)
        line_send(i, before, 0, 1, 4)
        got(plane(i, after, 1), SEM_B + i * 6 + 1)
        line_send(i, after, 1, 3, 5)
    for i in range(3):
        before, after = (own[i] + 3) % 4, (own[i] + 1) % 4
        got(plane(i, before, 1), SEM_B + i * 6 + 2)
        hand_over(i, 3)
        got(plane(i, after, 0), SEM_B + i * 6 + 3)
        hand_over(i, 1)
    for i in range(3):
        across = (own[i] + 2) % 4
        got(plane(i, across, 0), SEM_B + i * 6 + 4)
        got(plane(i, across, 1), SEM_B + i * 6 + 5)
        hand_over(i, 2)
    w_end(w_one, 0)
    w_start(w_line, 1, 4)
    gcopy.wait()
    for w in vcopies:
        w.wait()
    proj = jnp.zeros((512, 128), F32)
    for i in range(3):
        for d in range(4):
            line = (own[i] + d) % 4
            view = X.at[oc]
            if i == 0:
                view = view.at[line, :, :, :, cols(i)]
            elif i == 1:
                view = view.at[:, line, :, :, cols(i)]
            else:
                view = view.at[:, :, line, :, cols(i)]
            got(view, SEM_F + i * 4 + d)
        at, width = PIECES[i]
        for h in range(2):
            w = WGV[:, :, h * HALF + at : h * HALF + at + width].reshape(128, width)
            proj = proj + dot(X[h, :, :, :, :, at : at + width].reshape(512, width), w, NT)
    SP[...] = proj.reshape(64, 8, 128).astype(BF)

    for d in FAR:
        q = peer(d)
        send(SP.at[q], R1.at[e], SEM_P + q, SEM_P + e, (q, c)).start()

    def p_sent(k, _):
        q = lax.rem(e + 1 + k, 64)
        sent(SP.at[q], SEM_P + q)
        return 0

    pending.append(lambda: lax.fori_loop(0, 63, p_sent, 0))
    R1[e] = SP[e]

    loads["routes"].wait()
    loads["cw"].wait()
    lane8 = lax.broadcasted_iota(jnp.int32, (8, 128), 1)
    hit = jnp.zeros((8, 128), F32)
    wgt = jnp.zeros((8, 128), F32)
    rt = v["routes"][...]
    cwv = v["cw"][...]
    for k in range(6):
        eq = lane8 == rt[:, k : k + 1]
        hit = hit + jnp.where(eq, 1.0, 0.0)
        wgt = wgt + jnp.where(eq, cwv[:, k : k + 1], 0.0)
    before = (
        lax.broadcasted_iota(jnp.int32, (8, 8), 0) > lax.broadcasted_iota(jnp.int32, (8, 8), 1)
    ).astype(BF)
    slot = dot(before, hit.astype(BF))
    s0 = jnp.where(slot < 0.5, 1.0, 0.0)
    w1 = wgt.astype(BF).astype(F32)
    w2 = wgt - w1
    rows6 = jnp.concatenate(
        [hit * s0, hit * (1 - s0), w1 * s0, w1 * (1 - s0), w2 * s0, w2 * (1 - s0)], axis=0
    ).astype(BF)
    place = (
        lax.broadcasted_iota(jnp.int32, (128, 1024), 1) // 16
        == lax.broadcasted_iota(jnp.int32, (128, 1024), 0)
    ).astype(BF)
    six = dot(rows6, place)
    lane_r = lax.broadcasted_iota(jnp.int32, (8, 1024), 1)
    first = (lane_r // 8) % 2 == 0
    hsel = jnp.where(first, six[0:8], six[8:16])
    w1s = jnp.where(first, six[16:24], six[24:32])
    w2s = jnp.where(first, six[32:40], six[40:48])
    tile = lane_r % 8
    zero = jnp.zeros((8, 1024), F32)

    def diag(a):
        return jnp.concatenate([jnp.where(tile == j, a, zero) for j in range(8)], axis=0)

    DM[...] = jnp.concatenate([diag(hsel), jnp.zeros((64, 1024), F32)], axis=0).T.astype(BF)
    CM[...] = jnp.concatenate([diag(w1s), diag(w2s)], axis=0).astype(BF)
    for n in ("vt", "pv", "gg"):
        loads[n].wait()

    for d in FAR[::-1]:
        q = peer(d)
        got(R1.at[q], SEM_P + q)

    gates, values = [], []
    for t in range(16):
        r = [R1[4 * t + j].astype(F32) for j in range(4)]
        gates.append(lane_groups(r, lane8))
        values.append(pltpu.roll(lane_groups([r[3], r[0], r[1], r[2]], lane8), 96, 1))
    gate = jnp.concatenate(gates, axis=1)
    value = jnp.concatenate(values, axis=1)
    value_rows = value.astype(BF)
    v_conv = conv(v["pv"], value, v["vt"])
    mixed = (kept + v_conv * v_gain) * silu(gate)
    normed_groups = []
    for g in range(4):
        m = mixed[:, g * 512 : (g + 1) * 512]
        normed_groups.append(m * lax.rsqrt(jnp.mean(m * m, axis=1, keepdims=True) + EPSILON))
    mixer_rows = jnp.concatenate(normed_groups, axis=1) * v["gg"][...]
    M[x] = mixer_rows.astype(BF)

    for d in (2, 1, 3):
        send(M.at[x], M.at[x], SEM_M + xs[d], SEM_M + x, (peer((0, 0, d)), c)).start()
        pending.append(lambda d=d: sent(M.at[x], SEM_M + xs[d]))
    w_relay(w_line, 1, 4)
    for new, old, fresh in ((nv_o, "pv", value_rows), (ni_o, "pi", in_rows), (no_o, "po", out_rows)):
        new[0] = v[old][1]
        new[1] = v[old][2]
        new[2] = fresh

    u = v_conv * dt_w
    u1 = u.astype(BF).astype(F32)
    pad = jnp.zeros((104, 2048), F32)
    UT[...] = jnp.concatenate([u1, u1, u - u1, pad], axis=0).T.astype(BF)

    def st_step(b, _):
        bv = BV[...]
        b1 = bv.astype(BF).astype(F32)
        keep = lax.broadcasted_iota(jnp.int32, (8, 512), 0) == b
        zero = jnp.zeros((8, 512), F32)
        k1, k2 = jnp.where(keep, b1, zero), jnp.where(keep, bv - b1, zero)
        rhs = jnp.concatenate([k1, k2, k1, jnp.zeros((104, 512), F32)], axis=0).astype(BF)
        for g in range(4):
            outer = dot(UT[g * 512 : (g + 1) * 512, :], rhs[:, g * 128 : (g + 1) * 128])
            for h in range(8):
                sl = pl.ds(g * 512 + h * 64, 64)
                keep_h = DV[b, pl.ds(g * 8 + h, 1), :]
                st_o[b, sl, :] = keep_h * v["st"][b, sl, :] + outer[h * 64 : (h + 1) * 64]
        return 0

    lax.fori_loop(0, 8, st_step, 0)
    finish()
    for d in (1, 3, 2):
        got(M.at[xs[d]], SEM_M + xs[d])
    w_end(w_line, 4)
    part = dot(M[...].reshape(32, 2048), WM[...].reshape(512, 2048), NT)
    SQ[...] = part.reshape(4, 8, 512).astype(BF)
    mine = c * 4 + x
    for d in (2, 1, 3, 0):
        q = xs[d]
        for other in (oc, c):
            if d == 0 and other is c:
                continue
            k = SEM_Q + q * 2 + other
            send(SQ.at[q], R2.at[mine], k, SEM_Q + mine, (peer((0, 0, d)), other)).start()
            pending.append(lambda q=q, k=k: sent(SQ.at[q], k))
    R2[mine] = SQ[x]
    for d in (0, 1, 3, 2):
        for other in (oc, c):
            if d == 0 and other is c:
                continue
            k = other * 4 + xs[d]
            got(R2.at[k], SEM_Q + k)
    tiles = [None] * 16
    a = [
        (R2[xx].astype(F32) + R2[4 + xx].astype(F32)).astype(BF).astype(F32) for xx in range(4)
    ]
    for zz in range(4):
        for yy in range(4):
            moved = [
                b[:, zz * 128 : (zz + 1) * 128]
                if xx == yy
                else pltpu.roll(b[:, zz * 128 : (zz + 1) * 128], (32 * (xx - yy)) % 128, 1)
                for xx, b in enumerate(a)
            ]
            tiles[zz * 4 + yy] = lane_groups(moved, lane8)
    mixed_out = jnp.concatenate(tiles, axis=1)
    loads["g2"].wait()
    stream = (tok + mixed_out).astype(BF).astype(F32)
    ffn = rms(stream, v["g2"][...]).astype(BF)
    ff32 = ffn.astype(F32)

    half = jnp.where(c == 0, ff32[:, :HALF], ff32[:, HALF:])
    stacked = jnp.concatenate([half[:, j * 128 : (j + 1) * 128] for j in range(8)], axis=0)
    FF[...] = jnp.concatenate([stacked, jnp.zeros((64, 128), F32)], axis=0).astype(BF)
    SD[...] = dot(DM[...], FF[...]).reshape(64, 16, 128).astype(BF)

    for d in FAR:
        q = peer(d)
        send(SD.at[q], RX.at[c, e], SEM_X + q, SEM_X + e, (q, c)).start()

    def x_sent(k, _):
        q = lax.rem(e + 1 + k, 64)
        sent(SD.at[q], SEM_X + q)
        return 0

    pending.append(lambda: lax.fori_loop(0, 63, x_sent, 0))
    RX[c, e] = SD[e]

    for n in ("cg", "cu", "cd"):
        loads[n].wait()
    sh = (silu(dot(ffn, v["cg"][...])) * dot(ffn, v["cu"][...])).astype(BF)
    shared = dot(sh, v["cd"][...]).astype(BF)
    SHS[...] = shared
    send(SHS, SHR, SEM_SH, SEM_SH, (e, oc)).start()
    pending.append(lambda: sent(SHS, SEM_SH))
    for n in ("rg", "ru", "rd"):
        loads[n].wait()

    def x_plane(h, dz):
        return RX.at[h, pl.ds(pl.multiple_of(zs[dz] * 16, 16), 16)]

    for dz in (0, 1, 3, 2):
        for d in FAR[::-1]:
            if d[0] == dz:
                q = peer(d)
                got(RX.at[c, q], SEM_X + q)
        send(x_plane(c, dz), x_plane(c, dz), SEM_FX + dz, SEM_FX + dz, (e, oc)).start()
        pending.append(lambda dz=dz: sent(x_plane(c, dz), SEM_FX + dz))
    def rows_of(h):
        XF[...] = RX[h].astype(F32).reshape(1024, 128)
        return jnp.concatenate(
            [XF[pl.ds(j, 128, stride=8), :].astype(BF) for j in range(8)], axis=1
        )

    theirs = pl.ds(pl.multiple_of(oc * HALF, HALF), HALF)
    ours = pl.ds(pl.multiple_of(c * HALF, HALF), HALF)
    rows = rows_of(c)
    gate_sum = dot(rows, v["rg"][ours, :])
    up_sum = dot(rows, v["ru"][ours, :])
    for dz in (0, 1, 3, 2):
        got(x_plane(oc, dz), SEM_FX + dz)
    rows = rows_of(oc)
    gate_sum = gate_sum + dot(rows, v["rg"][theirs, :])
    up_sum = up_sum + dot(rows, v["ru"][theirs, :])
    hid = (silu(gate_sum) * up_sum).astype(BF)
    YS[...] = dot(hid, v["rd"][:, theirs]).astype(BF)
    send(YS, YR, SEM_YE, SEM_YE, (e, oc)).start()
    pending.append(lambda: sent(YS, SEM_YE))
    part_y = dot(hid, v["rd"][:, ours]).astype(BF).astype(F32)
    got(YR, SEM_YE)
    total_y = part_y + YR[...].astype(F32)
    for j in range(8):
        XF[pl.ds(j, 128, stride=8), :] = total_y[:, j * 128 : (j + 1) * 128]
    SY[...] = XF[...].reshape(64, 16, 128).astype(BF)

    for d in FAR:
        q = peer(d)
        send(SY.at[q], RY.at[e], SEM_Y + q, SEM_Y + e, (q, c)).start()

    def y_sent(k, _):
        q = lax.rem(e + 1 + k, 64)
        sent(SY.at[q], SEM_Y + q)
        return 0

    pending.append(lambda: lax.fori_loop(0, 63, y_sent, 0))
    RY[e] = SY[e]
    got(SHR, SEM_SH)
    resid = stream + (shared.astype(F32) + SHR[...].astype(F32))
    resid_half = jnp.where(c == 0, resid[:, :HALF], resid[:, HALF:])

    while len(pending) > 1:
        pending.pop(0)()
    both = jnp.zeros((128, 128), F32)
    for dz in (0, 1, 3, 2):
        for d in FAR[::-1]:
            if d[0] == dz:
                q = peer(d)
                got(RY.at[q], SEM_Y + q)
        lanes = pl.ds(pl.multiple_of(zs[dz] * 256, 256), 256)
        block = RY[pl.ds(pl.multiple_of(zs[dz] * 16, 16), 16)].reshape(256, 128)
        both = both + dot(CM[:, lanes], block)
    comb = both[0:64] + both[64:128]
    routed = jnp.concatenate([comb[j * 8 : (j + 1) * 8] for j in range(8)], axis=1)
    res = (resid_half + routed).astype(BF)
    RES[...] = res
    send(RES, RESR, SEM_RF, SEM_RF, (e, oc)).start()
    pending.append(lambda: sent(RES, SEM_RF))
    res_o[:, ours] = res
    got(RESR, SEM_RF)
    res_o[:, theirs] = RESR[...]
    finish()


def store_kernel(*refs):
    n = len(refs) // 2
    sem = refs[-1]
    copies = []
    for k in range(n):
        src, dst = refs[k], refs[n + k]
        if k == 1:
            copies += [(src.at[b], dst.at[b]) for b in range(8)]
        else:
            copies.append((src, dst))
    started = [pltpu.make_async_copy(a, b, sem.at[k]) for k, (a, b) in enumerate(copies)]
    for w in started:
        w.start()
    for w in started:
        w.wait()


def shards(
    tokens,
    mixer_norm_gain,
    gate_projection_weight,
    value_projection_weight,
    input_projection_weight,
    output_projection_weight,
    step_projection_weight,
    head_step_bias,
    head_decay_rate,
    extra_log_decay,
    value_taps,
    input_taps,
    output_taps,
    prior_values,
    prior_input_maps,
    prior_output_maps,
    head_skip_gain,
    group_norm_gain,
    mixer_output_weight,
    recurrent_state,
    expert_norm_gain,
    routes,
    chosen_expert_weight,
    routed_gate_weight,
    routed_up_weight,
    routed_down_weight,
    common_gate_weight,
    common_up_weight,
    common_down_weight,
):
    pv, pi, po = (
        jnp.transpose(a, (1, 0, 2)) for a in (prior_values, prior_input_maps, prior_output_maps)
    )
    state = recurrent_state.reshape(8, 2048, 128)
    vals = dict(
        tok=tokens,
        g1=mixer_norm_gain[None],
        wi=input_projection_weight,
        wo=output_projection_weight,
        wst=step_projection_weight.T,
        sb=head_step_bias[None],
        dr=head_decay_rate[None],
        eld=extra_log_decay,
        vt=value_taps,
        it=input_taps,
        ot=output_taps,
        pv=pv,
        pi=pi,
        po=po,
        hs=head_skip_gain[None],
        gg=group_norm_gain[None],
        g2=expert_norm_gain[None],
        routes=routes,
        cw=chosen_expert_weight,
        rg=routed_gate_weight[0],
        ru=routed_up_weight[0],
        rd=routed_down_weight[0],
        cg=common_gate_weight,
        cu=common_up_weight,
        cd=common_down_weight,
        st=state,
    )
    ins = [vals[n] for n in LOADED] + [
        jnp.transpose(gate_projection_weight, (1, 2, 0))[0],
        jnp.transpose(value_projection_weight, (1, 2, 0))[0],
        mixer_output_weight.T,
    ]
    vm = pltpu.VMEM
    scratch = [vm(vals[n].shape, vals[n].dtype) for n in LOADED] + [
        vm((2, 4, 4, 4, 8, HALF), BF),
        vm((4, 32, 2048), BF),
        vm((4, 4, 32, 2048), BF),
        vm((64, 8, 128), BF),
        vm((64, 8, 128), BF),
        vm((4, 8, 2048), BF),
        vm((4, 8, 512), BF),
        vm((8, 8, 512), BF),
        vm((64, 16, 128), BF),
        vm((2, 64, 16, 128), BF),
        vm((1024, 128), F32),
        vm((128, HALF), BF),
        vm((128, HALF), BF),
        vm((64, 16, 128), BF),
        vm((64, 16, 128), BF),
        vm((8, 2048), BF),
        vm((8, 2048), BF),
        vm((8, HALF), BF),
        vm((8, HALF), BF),
        vm((1024, 128), BF),
        vm((128, 1024), BF),
        vm((8, 2048), F32),
        vm((16, 512), BF),
        vm((128, 128), BF),
        vm((8, 512), F32),
        vm((8, 32, 128), F32),
        vm((2048, 128), BF),
        pltpu.SemaphoreType.DMA((len(LOADED) + 5,)),
        pltpu.SemaphoreType.DMA((SEM_COUNT,)),
        pltpu.SemaphoreType.DMA((SEM_COUNT,)),
    ]
    shapes = [
        ((8, 2048), BF),
        ((8, 2048, 128), F32),
        ((3, 8, 2048), BF),
        ((3, 8, 512), BF),
        ((3, 8, 512), BF),
    ]
    held = pl.pallas_call(
        layer_kernel,
        out_shape=[pltpu.VMEM(a, t) for a, t in shapes],
        in_specs=[pl.BlockSpec(memory_space=pltpu.HBM)] * len(ins),
        out_specs=[pl.BlockSpec(memory_space=pltpu.VMEM)] * 5,
        scratch_shapes=scratch,
        compiler_params=pltpu.CompilerParams(
            collective_id=0, has_side_effects=True, vmem_limit_bytes=50 * 2**20
        ),
    )(*ins)
    result, state_next, nv, ni, no = pl.pallas_call(
        store_kernel,
        out_shape=[jax.ShapeDtypeStruct(a, t) for a, t in shapes],
        in_specs=[pl.BlockSpec(memory_space=pl.ANY)] * 5,
        out_specs=[pl.BlockSpec(memory_space=pltpu.HBM)] * 5,
        scratch_shapes=[pltpu.SemaphoreType.DMA((12,))],
        compiler_params=pltpu.CompilerParams(vmem_limit_bytes=2**20),
    )(*held)
    return (
        result,
        state_next.reshape(8, 32, 64, 128),
        jnp.transpose(nv, (1, 0, 2)),
        jnp.transpose(ni, (1, 0, 2)),
        jnp.transpose(no, (1, 0, 2)),
    )


def solution(mesh):
    return jax.shard_map(
        shards,
        mesh=mesh,
        in_specs=(
            P("ep", None),
            P(),
            P(None, "tp", "ep"),
            P(None, "tp", "ep"),
            P(None, "tp"),
            P(None, "tp"),
            P(None, "tp"),
            P("tp"),
            P("tp"),
            P("ep", "tp"),
            P(None, "tp"),
            P(None, "tp"),
            P(None, "tp"),
            P("ep", None, "tp"),
            P("ep", None, "tp"),
            P("ep", None, "tp"),
            P("tp"),
            P("tp"),
            P("tp", "ep"),
            P("ep", "tp", None, None),
            P(),
            P("ep", None),
            P("ep", None),
            P("ep", None, "tp"),
            P("ep", None, "tp"),
            P("ep", "tp", None),
            P(None, "tp"),
            P(None, "tp"),
            P("tp", None),
        ),
        out_specs=(
            P("ep", None),
            P("ep", "tp", None, None),
            P("ep", None, "tp"),
            P("ep", None, "tp"),
            P("ep", None, "tp"),
        ),
        check_vma=False,
    )
```
